128 devices in a mesh: sp: 32 (over z, y, core), tp: 4 (over x).
Axes of the slice: x: 4, y: 4, z: 4, core: 2. Of those that a mesh axis runs over, the one named last changes fastest.
Arguments:
- mixer_value_projection: bfloat16 [24576, 2048], P('sp', 'tp'), may hold values from -6 to 6
- write_vectors_projected: bfloat16 [24576, 256], P('sp', 'tp'), may hold values from -6 to 6
- read_vectors_projected: bfloat16 [24576, 256], P('sp', 'tp'), may hold values from -6 to 6
- output_gate_projected: bfloat16 [24576, 2048], P('sp', 'tp'), may hold values from -6 to 6
- step_size_scores: float32 [24576, 32], P('sp', 'tp'), may hold values from -8 to 8
- position_decay_extra: float32 [24576, 32], P('sp', 'tp'), may hold values from -1 to 0
- step_size_bias: float32 [32], P('tp'), may hold values from -1 to 1
- head_decay_logarithm: float32 [32], P('tp'), may hold values from -14 to -3
- value_filter_taps: bfloat16 [4, 2048], P(None, 'tp'), may hold values from -3 to 3
- write_filter_taps: bfloat16 [4, 256], P(None, 'tp'), may hold values from -3 to 3
- read_filter_taps: bfloat16 [4, 256], P(None, 'tp'), may hold values from -3 to 3
- gated_group_norm_gain: float32 [2048], P('tp'), may hold values from 0.1 to 1.9
- mixer_output_weight: bfloat16 [2048, 2048], P('tp'), may hold values from -0.125 to 0.125
- residual: bfloat16 [24576, 2048], P('sp'), may hold values from -6 to 6
- feedforward_norm_gain: float32 [2048], replicated, may hold values from 0.1 to 1.9
- feedforward_gate_weight: bfloat16 [2048, 5632], P('sp', 'tp'), may hold values from -0.125 to 0.125
- feedforward_value_weight: bfloat16 [2048, 5632], P('sp', 'tp'), may hold values from -0.125 to 0.125
- gate_filter_taps: bfloat16 [3, 5632], P(None, 'tp'), may hold values from -3.5 to 3.5
- single_value_filter_taps: bfloat16 [3, 5632], P(None, 'tp'), may hold values from -3.5 to 3.5
- feedforward_down_weight: bfloat16 [5632, 2048], P('tp', 'sp'), may hold values from -0.078125 to 0.078125
Outputs:
- mixed: bfloat16 [24576, 2048], P(('sp', 'tp'))
The draws below stay inside these ranges and needn't reach their ends.
All inputs are finite; a program needn't handle non-finite values.
Results may differ from the reference program's by a relative error of at most 0.012.
Values may be sent and summed in bfloat16 or wider, within the bound.
A program may use at most 192 MiB of HBM per device.

```python
import jax
import jax.numpy as jnp
from jax import lax

D = 2048
HEADS = 32
HEAD = 64
GROUPS = 4
STATE = 64
FF = 5632
TOK_DEV = 768
BLOCK = 128
CONV_MIX = 4
CONV_FFN = 3
INNER = 2048
SEQ = 24576


def draw_step_size_scores(key, part):
    first, second = jax.random.split(jax.random.fold_in(key, 11))
    block_total = SEQ // TOK_DEV
    base = jax.random.normal(first, (SEQ, HEADS), jnp.float32)
    shifts = jax.random.uniform(second, (block_total, 1, HEADS), jnp.float32, -1.5, 1.5)
    return (base.reshape(block_total, TOK_DEV, HEADS) + shifts).reshape(SEQ, HEADS)


def draw_head_decay_logarithm(key, part):
    first, second, third = jax.random.split(jax.random.fold_in(key, 12), 3)
    share = 0.5
    slowly = jax.random.uniform(first, (HEADS,), jnp.float32) < share
    slow_rate = jnp.log(jax.random.uniform(second, (HEADS,), jnp.float32, 0.4, 1.0) / SEQ)
    fast_rate = jax.random.uniform(third, (HEADS,), jnp.float32, jnp.log(1.0 / 60.0), jnp.log(1.0 / 25.0))
    return jnp.where(slowly, slow_rate, fast_rate)


def draw_position_decay_extra(key, part):
    first, second = jax.random.split(jax.random.fold_in(key, 13))
    places = jax.random.randint(first, (3,), 0, SEQ)
    losses = jnp.log(jax.random.uniform(second, (3, HEADS), jnp.float32, 0.5, 0.8))
    positions = jnp.arange(SEQ)
    hits = (positions[:, None] == places[None, :]).astype(jnp.float32)
    return jnp.sum(hits[:, :, None] * losses[None, :, :], axis=1)


def block_levels(rng, dims, cuts, smallest, top_value):
    level = 1.0
    for position, parts in cuts:
        heights = jax.random.uniform(jax.random.fold_in(jax.random.fold_in(rng, 6), position), (parts,), jnp.float32, smallest / len(cuts), top_value / len(cuts))
        level = level * jnp.repeat(jnp.exp(heights), dims[position] // parts).reshape((-1,) + (1,) * (len(dims) - 1 - position))
    return level


def scatter_about(own_key, extent, deviation, bound, pieces=(), held_as=jnp.bfloat16):
    loudness = block_levels(own_key, extent, pieces, -0.22, 0.18) if pieces else 1.0
    array = jax.random.normal(own_key, extent, jnp.float32) * deviation * loudness
    return jnp.minimum(jnp.maximum(array, -bound), bound).astype(held_as)


def setup_inputs(seed: int = 0) -> dict:
    streams_of = jax.random.split(jax.random.key(seed), 21)
    mixer_value_projection = scatter_about(streams_of[0], (SEQ, INNER), 1.0, 6.0, ((0, 32), (1, 4)))
    write_vectors_projected = scatter_about(streams_of[1], (SEQ, GROUPS * STATE), 1.0, 6.0, ((0, 32), (1, 4)))
    read_vectors_projected = scatter_about(streams_of[2], (SEQ, GROUPS * STATE), 1.0, 6.0, ((0, 32), (1, 4)))
    output_gate_projected = scatter_about(streams_of[3], (SEQ, INNER), 1.0, 6.0, ((0, 32), (1, 4)))
    step_size_scores = draw_step_size_scores(jax.random.fold_in(streams_of[20], 71), 0)
    position_decay_extra = draw_position_decay_extra(jax.random.fold_in(streams_of[20], 71), 0)
    step_size_bias = jnp.clip(jax.random.uniform(streams_of[6], (HEADS,), jnp.float32, -1.0, 1.0) * block_levels(streams_of[6], (HEADS,), ((0, 4),), -0.4, 0.0), -1.0, 1.0)
    head_decay_logarithm = draw_head_decay_logarithm(jax.random.fold_in(streams_of[20], 71), 0)
    value_filter_taps = scatter_about(streams_of[8], (CONV_MIX, INNER), CONV_MIX ** -0.5, 3.0, ((1, 4),))
    write_filter_taps = scatter_about(streams_of[9], (CONV_MIX, GROUPS * STATE), CONV_MIX ** -0.5, 3.0, ((1, 4),))
    read_filter_taps = scatter_about(streams_of[10], (CONV_MIX, GROUPS * STATE), CONV_MIX ** -0.5, 3.0, ((1, 4),))
    gated_group_norm_gain = jnp.clip(1.0 + 0.18 * jax.random.normal(streams_of[11], (INNER,), jnp.float32), 0.1, 1.9)
    mixer_output_weight = scatter_about(streams_of[12], (INNER, D), INNER ** -0.5, 0.125, ((0, 4),))
    residual = scatter_about(streams_of[13], (SEQ, D), 1.0, 6.0, ((0, 32),))
    feedforward_norm_gain = jnp.clip(1.0 + 0.18 * jax.random.normal(streams_of[14], (D,), jnp.float32), 0.1, 1.9)
    feedforward_gate_weight = scatter_about(streams_of[15], (D, FF), D ** -0.5, 0.125, ((0, 32), (1, 4)))
    feedforward_value_weight = scatter_about(streams_of[16], (D, FF), D ** -0.5, 0.125, ((0, 32), (1, 4)))
    gate_filter_taps = scatter_about(streams_of[17], (CONV_FFN, FF), CONV_FFN ** -0.5, 3.5, ((1, 4),))
    single_value_filter_taps = scatter_about(streams_of[18], (CONV_FFN, FF), CONV_FFN ** -0.5, 3.5, ((1, 4),))
    feedforward_down_weight = scatter_about(streams_of[19], (FF, D), FF ** -0.5, 0.078125, ((0, 4), (1, 32)))
    return {"mixer_value_projection": mixer_value_projection, "write_vectors_projected": write_vectors_projected, "read_vectors_projected": read_vectors_projected, "output_gate_projected": output_gate_projected, "step_size_scores": step_size_scores, "position_decay_extra": position_decay_extra, "step_size_bias": step_size_bias, "head_decay_logarithm": head_decay_logarithm, "value_filter_taps": value_filter_taps, "write_filter_taps": write_filter_taps, "read_filter_taps": read_filter_taps, "gated_group_norm_gain": gated_group_norm_gain, "mixer_output_weight": mixer_output_weight, "residual": residual, "feedforward_norm_gain": feedforward_norm_gain, "feedforward_gate_weight": feedforward_gate_weight, "feedforward_value_weight": feedforward_value_weight, "gate_filter_taps": gate_filter_taps, "single_value_filter_taps": single_value_filter_taps, "feedforward_down_weight": feedforward_down_weight}


epsilon = 1e-06

def causal_taps(current, kernel):
    tap_count = kernel.shape[0]
    length = current.shape[0]
    padded = jnp.concatenate([jnp.zeros((tap_count - 1, current.shape[1]), current.dtype), current], 0).astype(jnp.float32)
    result = jnp.zeros((length, current.shape[1]), jnp.float32)
    for offset in range(tap_count):
        result = result + kernel[offset].astype(jnp.float32) * padded[offset:offset + length]
    return result

def channel_norm(stream, gain):
    floats = stream.astype(jnp.float32)
    scaled = floats * lax.rsqrt(lax.optimization_barrier(jnp.mean(floats * floats, axis=-1, keepdims=True)) + epsilon)
    return (scaled * gain).astype(jnp.bfloat16)

def reference(mixer_value_projection, write_vectors_projected, read_vectors_projected, output_gate_projected, step_size_scores, position_decay_extra, step_size_bias, head_decay_logarithm, value_filter_taps, write_filter_taps, read_filter_taps, gated_group_norm_gain, mixer_output_weight, residual, feedforward_norm_gain, feedforward_gate_weight, feedforward_value_weight, gate_filter_taps, single_value_filter_taps, feedforward_down_weight):
    per_group = HEADS // GROUPS
    x_conv = jax.nn.silu(causal_taps(mixer_value_projection, value_filter_taps)).astype(jnp.bfloat16)
    write_conv = jax.nn.silu(causal_taps(write_vectors_projected, write_filter_taps)).astype(jnp.bfloat16)
    read_conv = jax.nn.silu(causal_taps(read_vectors_projected, read_filter_taps)).astype(jnp.bfloat16)
    step_size_head = jax.nn.softplus(step_size_scores + step_size_bias)
    logarithm_decay_rate = -step_size_head * jnp.exp(head_decay_logarithm) + position_decay_extra
    scaled = (x_conv.astype(jnp.float32).reshape(SEQ, HEADS, HEAD) * step_size_head[:, :, None]).astype(jnp.bfloat16)
    block_count = SEQ // BLOCK
    value_blocks = scaled.reshape(block_count, BLOCK, GROUPS, per_group, HEAD)
    write_blocks = write_conv.reshape(block_count, BLOCK, GROUPS, STATE)
    read_blocks = read_conv.reshape(block_count, BLOCK, GROUPS, STATE)
    log_blocks = logarithm_decay_rate.reshape(block_count, BLOCK, HEADS)
    causal = jnp.tril(jnp.ones((BLOCK, BLOCK), dtype=jnp.bool_))

    def block_step(carried, inputs):
        value_rows, write_rows, read_rows, log_rows = inputs
        running = jnp.cumsum(log_rows, axis=0)
        by_head = running.T
        spread = by_head[:, :, None] - by_head[:, None, :]
        decays = jnp.exp(jnp.where(causal, spread, -jnp.inf)).reshape(GROUPS, per_group, BLOCK, BLOCK)
        scores = jnp.einsum('lgn,sgn->gls', read_rows.astype(jnp.float32), write_rows.astype(jnp.float32))
        weights = (scores[:, None] * decays).astype(jnp.bfloat16)
        inside = jnp.einsum('grls,sgrp->lgrp', weights.astype(jnp.float32), value_rows.astype(jnp.float32))
        entering = jnp.einsum('lgn,grnp->lgrp', read_rows.astype(jnp.float32), carried, precision=lax.Precision.HIGHEST)
        entering = entering * jnp.exp(running).reshape(BLOCK, GROUPS, per_group)[..., None]
        tails = jnp.exp(by_head[:, -1:] - by_head).T.reshape(BLOCK, GROUPS, per_group)
        tailed = (value_rows.astype(jnp.float32) * tails[..., None]).astype(jnp.bfloat16)
        fresh = jnp.einsum('sgn,sgrp->grnp', write_rows.astype(jnp.float32), tailed.astype(jnp.float32))
        advanced = carried * jnp.exp(running[-1]).reshape(GROUPS, per_group)[..., None, None] + fresh
        return (advanced, inside + entering)
    start_state = jnp.zeros((GROUPS, per_group, STATE, HEAD), jnp.float32)
    outputs = lax.scan(block_step, start_state, (value_blocks, write_blocks, read_blocks, log_blocks))[1]
    mixer = outputs.reshape(SEQ, INNER)
    gated = (mixer * jax.nn.silu(output_gate_projected.astype(jnp.float32))).reshape(SEQ, GROUPS, INNER // GROUPS)
    gated = gated * lax.rsqrt(lax.optimization_barrier(jnp.mean(gated * gated, axis=-1, keepdims=True)) + epsilon)
    normed = (gated.reshape(SEQ, INNER) * gated_group_norm_gain).astype(jnp.bfloat16)
    stream = (residual.astype(jnp.float32) + jnp.dot(normed, mixer_output_weight, preferred_element_type=jnp.float32)).astype(jnp.bfloat16)
    ffn_in = channel_norm(stream, feedforward_norm_gain)
    gate_rows = jnp.dot(ffn_in, feedforward_gate_weight, preferred_element_type=jnp.float32).astype(jnp.bfloat16)
    value_rows = jnp.dot(ffn_in, feedforward_value_weight, preferred_element_type=jnp.float32).astype(jnp.bfloat16)
    hidden = (jax.nn.silu(causal_taps(gate_rows, gate_filter_taps)) * causal_taps(value_rows, single_value_filter_taps)).astype(jnp.bfloat16)
    down = jnp.dot(hidden, feedforward_down_weight, preferred_element_type=jnp.float32)
    return (stream.astype(jnp.float32) + down).astype(jnp.bfloat16)
```

```python
import functools

import jax
import jax.numpy as jnp
from jax import lax
from jax.experimental import pallas as pl
from jax.experimental.pallas import tpu as pltpu
from jax.sharding import Mesh
from jax.sharding import PartitionSpec as P

SP = ("sp_0", "sp_1", "sp_2")
SP_TP = ("sp_0", "sp_1", "sp_2", "tp")
MESH = pl.DeviceIdType.MESH
EPS = 1e-06
F32 = jnp.float32
BF16 = jnp.bfloat16
HI = lax.Precision.HIGHEST

ROWS = 768
BLOCK = 128
BLOCKS = 6
HEADS = 8
INNER = 512
WIDTH = 2048
HIDDEN = 1408
SHARE = 192


def silu(v):
    return v / (1.0 + jnp.exp(-v))


def dot(a, b):
    return jnp.dot(a, b, preferred_element_type=F32)


def kernel(
    xv, wrt, rdt, og, sct, ext, bias, hlog, vtap, bctap, ggain, wout, res, fgain, gw, vw, gtap, vtap2, dwt,
    out,
    xs, bct, ogs, st_s, cum_s, bt_s, c_s, sc_s, ecx_s, ins_s, lb_s, pre_s, stv, plog,
    m1, r1, r2, r3, inc,
    ng, stream, fin, wof, gvd, hid, sbuf, ra, rb, rl, rr, own,
    lsem, hsend, hrecv, xsend, xrecv, ssend, srecv, wsend, wrecv, asend, arecv, qsend, qrecv,
):
    z = lax.axis_index("sp_0")
    y = lax.axis_index("sp_1")
    c = lax.axis_index("sp_2")
    x = lax.axis_index("tp")
    sp = z * 8 + y * 2 + c

    def at_sp(s):
        return ((s // 8) % 4, (s // 2) % 4, s % 2, x)

    nxt = at_sp(sp + 1)
    prv = at_sp(sp + 31)
    partner = (z, y, 1 - c, x)

    def dev_x(d):
        return (z, y, c, (x + d + 4) % 4)

    def dev_y(d):
        return (z, (y + d) % 4, c, x)

    def dev_z(d):
        return ((z + d) % 4, y, c, x)

    def dev1(d):
        return ((z + 4 + d * c) % 4, (y + 4 + d * (1 - c)) % 4, c, x)

    def dev2(d):
        return ((z + 4 + d * (1 - c)) % 4, (y + 4 + d * c) % 4, c, x)

    ca = c * z + (1 - c) * y
    cb = c * y + (1 - c) * z

    def item(da, db):
        return ((ca + 4 + da) % 4) * (2 + 6 * c) + ((cb + 4 + db) % 4) * (8 - 6 * c) + c

    def remote(src, dst, ss, rs, dev):
        return pltpu.make_async_remote_copy(
            src_ref=src, dst_ref=dst, send_sem=ss, recv_sem=rs, device_id=dev, device_id_type=MESH
        )

    loads = [
        pltpu.make_async_copy(xv, xs.at[pl.ds(16, ROWS)], lsem.at[0]),
        pltpu.make_async_copy(wrt, bct.at[pl.ds(0, 64), pl.ds(128, ROWS)], lsem.at[1]),
        pltpu.make_async_copy(rdt, bct.at[pl.ds(64, 64), pl.ds(128, ROWS)], lsem.at[2]),
        pltpu.make_async_copy(gw, gvd.at[sp, 0], lsem.at[3]),
        pltpu.make_async_copy(vw, gvd.at[sp, 1], lsem.at[4]),
        pltpu.make_async_copy(dwt, gvd.at[sp, 2], lsem.at[5]),
        pltpu.make_async_copy(og, ogs, lsem.at[6]),
        pltpu.make_async_copy(wout, wof.at[0], lsem.at[7]),
        pltpu.make_async_copy(res, stream, lsem.at[8]),
    ]
    for load in loads:
        load.start()

    barrier = pltpu.get_barrier_semaphore()
    peers = [partner, nxt, prv]
    for d in (1, 2, 3):
        peers += [dev_x(d), dev_y(d), dev_z(d)]
    for peer in peers:
        pl.semaphore_signal(barrier, inc=1, device_id=peer, device_id_type=MESH)
    pl.semaphore_wait(barrier, len(peers))

    pending = []

    def start(copy):
        copy.start()
        pending.append(copy)

    halo = [
        remote(xv.at[pl.ds(ROWS - 16, 16)], xs.at[pl.ds(0, 16)], hsend.at[0], hrecv.at[0], nxt),
        remote(wrt.at[:, pl.ds(ROWS - 128, 128)], bct.at[pl.ds(0, 64), pl.ds(0, 128)], hsend.at[1], hrecv.at[1], nxt),
        remote(rdt.at[:, pl.ds(ROWS - 128, 128)], bct.at[pl.ds(64, 64), pl.ds(0, 128)], hsend.at[2], hrecv.at[2], nxt),
    ]

    @pl.when(sp < 31)
    def _():
        for h in halo:
            h.start()

    @pl.when(sp == 0)
    def _():
        xs[pl.ds(0, 16), :] = jnp.zeros((16, INNER), BF16)
        bct[:, pl.ds(0, 128)] = jnp.zeros((128, 128), BF16)
        fin[pl.ds(0, 16), :] = jnp.zeros((16, WIDTH), BF16)

    for r in (1, 2, 3):
        start(remote(wout.at[sp], wof.at[r, sp], xsend.at[r - 1], xrecv.at[r - 1], dev_x(-r)))

    def full(batch, k):
        if batch == 0:
            return wof.at[pl.ds(1, 3), k]
        if batch == 1:
            return gvd.at[k, pl.ds(0, 2)]
        return gvd.at[k, 2]

    def half(batch, k, side):
        if batch == 0:
            return wof.at[pl.ds(1, 3), k, :, pl.ds(1024 * side, 1024)]
        if batch == 1:
            return gvd.at[k, side]
        return gvd.at[k, 2, pl.ds(32 * side, 32)]

    def send(batch, ref, sem, dev):
        start(remote(ref, ref, wsend.at[batch, sem], wrecv.at[batch, sem], dev))

    def arrive(batch, ref, sem):
        remote(ref, ref, wsend.at[batch, sem], wrecv.at[batch, sem], partner).wait_recv()

    def to_partner(batch, k):
        ref = full(batch, k)
        start(remote(ref, ref, wsend.at[batch, 20 + k // 2], wrecv.at[batch, 20 + k // 2], partner))

    order = (0, -1, 1, 2)

    def first_sends(batch):
        k = item(0, 0)
        send(batch, full(batch, k), 1, dev1(-1))
        send(batch, full(batch, k), 0, dev1(1))
        second_sends(batch, 0)

    def second_sends(batch, j):
        k = item(order[j], 0)
        send(batch, full(batch, k), 4 + 4 * j + 1, dev2(-1))
        send(batch, full(batch, k), 4 + 4 * j, dev2(1))
        to_partner(batch, k)

    def first_events(batch):
        k = item(-1, 0)
        arrive(batch, full(batch, k), 0)
        send(batch, half(batch, k, 0), 2, dev1(1))
        k2 = item(1, 0)
        arrive(batch, full(batch, k2), 1)
        send(batch, half(batch, k2, 1), 3, dev1(-1))
        second_sends(batch, 1)
        second_sends(batch, 2)

    def third_event(batch):
        k = item(2, 0)
        arrive(batch, half(batch, k, 0), 2)
        arrive(batch, half(batch, k, 1), 3)
        second_sends(batch, 3)

    def second_events(batch, j):
        base = 4 + 4 * j
        k = item(order[j], -1)
        arrive(batch, full(batch, k), base)
        send(batch, half(batch, k, 0), base + 2, dev2(1))
        to_partner(batch, k)
        k = item(order[j], 1)
        arrive(batch, full(batch, k), base + 1)
        send(batch, half(batch, k, 1), base + 3, dev2(-1))
        to_partner(batch, k)

    def last_events(batch, j):
        base = 4 + 4 * j
        k = item(order[j], 2)
        arrive(batch, half(batch, k, 0), base + 2)
        arrive(batch, half(batch, k, 1), base + 3)
        to_partner(batch, k)

    def from_partner(batch):
        for i in range(16):
            arrive(batch, full(batch, 2 * i + 1 - c), 20 + i)

    for i in (3, 4, 5):
        loads[i].wait()
    for batch in (1, 2):
        k = item(0, 0)
        send(batch, full(batch, k), 1, dev1(-1))
        send(batch, full(batch, k), 0, dev1(1))

    head = lax.broadcasted_iota(jnp.int32, (HEADS, 1), 0)
    bias_c = jnp.zeros((HEADS, 1), F32)
    rate_c = jnp.zeros((HEADS, 1), F32)
    for h in range(HEADS):
        bias_c = jnp.where(head == h, bias[h], bias_c)
        rate_c = jnp.where(head == h, hlog[h], rate_c)
    rate_c = jnp.exp(rate_c)
    v = sct[...] + bias_c
    step = jnp.maximum(v, 0.0) + jnp.log1p(jnp.exp(-jnp.abs(v)))
    logd = -step * rate_c + ext[...]
    row_i = lax.broadcasted_iota(jnp.int32, (BLOCK, BLOCK), 0)
    col_i = lax.broadcasted_iota(jnp.int32, (BLOCK, BLOCK), 1)
    upper = (row_i <= col_i).astype(F32)
    for b in range(BLOCKS):
        st_s[b] = step[:, b * BLOCK : (b + 1) * BLOCK]
        cum_s[b] = jnp.dot(
            logd[:, b * BLOCK : (b + 1) * BLOCK], upper, preferred_element_type=F32, precision=HI
        )

    def expand(value):
        spread = (
            lax.broadcasted_iota(jnp.int32, (HEADS, INNER), 1) // 64
            == lax.broadcasted_iota(jnp.int32, (HEADS, INNER), 0)
        ).astype(F32)
        return jnp.dot(value.T, spread, preferred_element_type=F32, precision=HI)

    loads[0].wait()
    loads[1].wait()
    loads[2].wait()

    @pl.when(sp > 0)
    def _():
        for h in halo:
            h.wait_recv()

    stv[...] = jnp.zeros_like(stv)
    plog[...] = jnp.zeros_like(plog)
    vt = vtap[...].astype(F32)
    bt = bctap[...].astype(F32)

    def local(b, _):
        r0 = pl.multiple_of(b * BLOCK, BLOCK)
        rows = xs[pl.ds(r0, BLOCK + 16), :].astype(F32)
        conv = vt[3:4] * rows
        for j in range(3):
            conv = conv + vt[j : j + 1] * pltpu.roll(rows, 3 - j, 0)
        xc = silu(conv[16:]).astype(BF16).astype(F32)
        lanes = bct[:, pl.ds(r0, 2 * BLOCK)].astype(F32)
        conv2 = bt[:, 3:4] * lanes
        for j in range(3):
            conv2 = conv2 + bt[:, j : j + 1] * pltpu.roll(lanes, 3 - j, 1)
        bc = silu(conv2[:, BLOCK:])
        wt = bc[:64].astype(BF16)
        rd = bc[64:].T.astype(BF16)
        bt_s[b] = wt
        c_s[b] = rd
        cumx = expand(cum_s[b])
        stepx = expand(st_s[b])
        last = cumx[BLOCK - 1 : BLOCK]
        scaled = (xc * stepx).astype(BF16)
        sc_s[pl.ds(r0, BLOCK), :] = scaled
        tailed = (scaled.astype(F32) * jnp.exp(last - cumx)).astype(BF16)
        ecx_s[pl.ds(r0, BLOCK), :] = jnp.exp(cumx)
        fresh = dot(wt, tailed)
        lb_s[b] = stv[...]
        pre_s[b] = plog[...]
        stv[...] = stv[...] * jnp.exp(last) + fresh
        plog[...] = plog[...] + last
        return 0

    def inner(b, _):
        r0 = pl.multiple_of(b * BLOCK, BLOCK)
        s = dot(c_s[b], bt_s[b])
        cum = cum_s[b]
        cumt = cum.T
        causal = (
            lax.broadcasted_iota(jnp.int32, (BLOCK, BLOCK), 0)
            >= lax.broadcasted_iota(jnp.int32, (BLOCK, BLOCK), 1)
        )
        low = lax.broadcasted_iota(jnp.int32, (BLOCK, BLOCK), 1) < 64
        for p in range(HEADS // 2):
            rhs = sc_s[pl.ds(r0, BLOCK), pl.ds(p * 128, 128)]
            parts = []
            for h in (2 * p, 2 * p + 1):
                spread = jnp.where(causal, cumt[:, h : h + 1] - cum[h : h + 1, :], -jnp.inf)
                parts.append(dot((s * jnp.exp(spread)).astype(BF16), rhs))
            ins_s[pl.ds(r0, BLOCK), pl.ds(p * 128, 128)] = jnp.where(low, parts[0], parts[1])
        return 0

    def put(ref, decay, state):
        ref[pl.ds(0, 64), :] = state.astype(BF16)
        d = jnp.broadcast_to(decay, (16, INNER))
        high = d.astype(BF16)
        ref[pl.ds(64, 16), :] = high
        ref[pl.ds(80, 16), :] = (d - high.astype(F32)).astype(BF16)

    def take(ref):
        decay = ref[pl.ds(64, 16), :].astype(F32) + ref[pl.ds(80, 16), :].astype(F32)
        return decay[0:1], ref[pl.ds(0, 64), :].astype(F32)

    def wait_pieces():
        for r in (1, 2, 3):
            remote(wout.at[sp], wof.at[r, sp], xsend.at[r - 1], xrecv.at[r - 1], dev_x(-r)).wait_recv()

    lax.fori_loop(0, 3, local, 0)
    wait_pieces()
    first_sends(0)
    lax.fori_loop(3, 6, local, 0)

    put(m1, jnp.exp(plog[...]), stv[...])
    first_events(0)
    start(remote(m1, r1, ssend.at[0], srecv.at[0], partner))
    lax.fori_loop(0, 3, inner, 0)
    remote(m1, r1, ssend.at[0], srecv.at[0], partner).wait_recv()
    d_own, s_own = jnp.exp(plog[...]), stv[...]
    d_par, s_par = take(r1)
    is_first = c == 0
    chip_d = d_own * d_par
    chip_s = jnp.where(is_first, s_own * d_par + s_par, s_par * d_own + s_own)
    put(r2.at[y], chip_d, chip_s)
    third_event(0)
    for d in (1, 2, 3):
        start(remote(r2.at[y], r2.at[y], ssend.at[d], srecv.at[d], dev_y(d)))
    lax.fori_loop(3, 6, inner, 0)
    for j in (0, 1):
        second_events(0, j)
    for d in (1, 2, 3):
        src = (y + 4 - d) % 4
        remote(r2.at[src], r2.at[src], ssend.at[d], srecv.at[d], dev_y(d)).wait_recv()
    row_d, row_s = take(r2.at[0])
    exc_d = jnp.where(y > 0, row_d, 1.0)
    exc_s = jnp.where(y > 0, row_s, 0.0)
    for i in (1, 2, 3):
        di, si = take(r2.at[i])
        row_s = row_s * di + si
        row_d = row_d * di
        exc_s = jnp.where(y > i, exc_s * di + si, exc_s)
        exc_d = jnp.where(y > i, exc_d * di, exc_d)
    put(r3.at[z], row_d, row_s)
    inc[0] = exc_s
    inc[1] = jnp.broadcast_to(exc_d, (64, INNER))
    for j in (2, 3):
        second_events(0, j)
    for d in (1, 2, 3):
        start(remote(r3.at[z], r3.at[z], ssend.at[3 + d], srecv.at[3 + d], dev_z(d)))
    for j in range(4):
        last_events(0, j)
    for d in (1, 2, 3):
        src = (z + 4 - d) % 4
        remote(r3.at[src], r3.at[src], ssend.at[3 + d], srecv.at[3 + d], dev_z(d)).wait_recv()
    acc = jnp.zeros((64, INNER), F32)
    for i in (0, 1, 2):
        di, si = take(r3.at[i])
        acc = jnp.where(z > i, acc * di + si, acc)
    acc = acc * inc[1] + inc[0]
    d_par, s_par = take(r1)
    inc[0] = jnp.where(is_first, acc, acc * d_par + s_par)

    for batch in (1, 2):
        second_sends(batch, 0)
        first_events(batch)
        third_event(batch)

    loads[6].wait()
    gain = ggain[...]

    def block_of(i):
        return (i + 4) % 6

    def rows_of(i):
        return pl.multiple_of(block_of(i) * BLOCK, BLOCK)

    def ng_full(r, i):
        return ng.at[r, pl.ds(rows_of(i), BLOCK)]

    def ng_half(r, i, side):
        return ng.at[r, pl.ds(pl.multiple_of(rows_of(i) + 64 * side, 64), 64)]

    def ag_right(i):
        return remote(ng_full(0, i), ng_full(3, i), asend.at[0, i], arecv.at[0, i], dev_x(1))

    def ag_left(i):
        return remote(ng_full(0, i), ng_full(1, i), asend.at[1, i], arecv.at[1, i], dev_x(-1))

    def ag_forward_right(i):
        return remote(ng_half(3, i, 0), ng_half(2, i, 0), asend.at[2, i], arecv.at[2, i], dev_x(1))

    def ag_forward_left(i):
        return remote(ng_half(1, i, 1), ng_half(2, i, 1), asend.at[3, i], arecv.at[3, i], dev_x(-1))

    def final(i, _):
        b = block_of(i)
        r0 = rows_of(i)
        state = lb_s[b] + inc[0] * jnp.exp(pre_s[b])
        ent = dot(c_s[b], state.astype(BF16))
        m = ins_s[pl.ds(r0, BLOCK), :] + ecx_s[pl.ds(r0, BLOCK), :] * ent
        g = m * silu(ogs[pl.ds(r0, BLOCK), :].astype(F32))
        scale = lax.rsqrt(jnp.mean(g * g, axis=-1, keepdims=True) + EPS)
        ng[0, pl.ds(r0, BLOCK), :] = (g * scale * gain).astype(BF16)

        @pl.when(i > 0)
        def _():
            ag_right(i - 1).start()
            ag_left(i - 1).start()

        return 0

    lax.fori_loop(0, BLOCKS, final, 0)
    for j in range(4):
        second_events(1, j)
    ag_right(BLOCKS - 1).start()
    ag_left(BLOCKS - 1).start()
    loads[7].wait()
    loads[8].wait()
    from_partner(0)
    fg = fgain[...]

    def project(g):
        for i in (2 * g, 2 * g + 1):
            ag_right(i).wait_recv()
            ag_forward_right(i).start()
            ag_left(i).wait_recv()
            ag_forward_left(i).start()
        for i in (2 * g, 2 * g + 1):
            ag_forward_right(i).wait_recv()
            ag_forward_left(i).wait_recv()
        r0 = ((g + 2) % 3) * 256

        def tile(n, total):
            n0 = pl.multiple_of(n * 256, 256)
            part = dot(ng[0, pl.ds(r0, 256), :], wof[0, :, :, pl.ds(n0, 256)].reshape(INNER, 256))
            for r in (1, 2, 3):
                part = part + dot(
                    ng[r, pl.ds(r0, 256), :], wof[r, :, :, pl.ds(n0, 256)].reshape(INNER, 256)
                )
            s = (stream[pl.ds(r0, 256), pl.ds(n0, 256)].astype(F32) + part).astype(BF16)
            stream[pl.ds(r0, 256), pl.ds(n0, 256)] = s
            sf = s.astype(F32)
            return total + jnp.sum(sf * sf, axis=-1, keepdims=True)

        total = lax.fori_loop(0, 8, tile, jnp.zeros((256, 1), F32))
        scale = lax.rsqrt(total * (1.0 / WIDTH) + EPS)

        def norm(n, _):
            n0 = pl.multiple_of(n * 256, 256)
            sf = stream[pl.ds(r0, 256), pl.ds(n0, 256)].astype(F32)
            fin[pl.ds(16 + r0, 256), pl.ds(n0, 256)] = (
                sf * scale * fgain[:, pl.ds(n0, 256)]
            ).astype(BF16)
            return 0

        lax.fori_loop(0, 8, norm, 0)

    project(0)
    rim = remote(fin.at[pl.ds(ROWS, 16)], fin.at[pl.ds(0, 16)], hsend.at[3], hrecv.at[3], nxt)
    for j in range(4):
        last_events(1, j)

    @pl.when(sp < 31)
    def _():
        rim.start()

    project(1)
    for j in range(4):
        second_events(2, j)
    project(2)
    for j in range(4):
        last_events(2, j)

    @pl.when(sp > 0)
    def _():
        rim.wait_recv()

    from_partner(1)
    from_partner(2)

    def feed(d, store):
        f0 = pl.multiple_of(d * SHARE, 64)

        def tile(n, _):
            n0 = pl.multiple_of(n * 128, 128)
            w = jnp.concatenate(
                [
                    gvd[:, 0, :, pl.ds(n0, 128)].reshape(WIDTH, 128),
                    gvd[:, 1, :, pl.ds(n0, 128)].reshape(WIDTH, 128),
                ],
                axis=1,
            )
            u = dot(fin[pl.ds(f0, SHARE + 16), :], w).astype(BF16).astype(F32)
            taps = jnp.concatenate(
                [gtap[:, pl.ds(n0, 128)].astype(F32), vtap2[:, pl.ds(n0, 128)].astype(F32)], axis=1
            )
            conv = taps[2:3] * u
            for j in range(2):
                conv = conv + taps[j : j + 1] * pltpu.roll(u, 2 - j, 0)
            conv = conv[16:]
            hid[:, pl.ds(n0, 128)] = (silu(conv[:, :128]) * conv[:, 128:]).astype(BF16)
            return 0

        lax.fori_loop(0, HIDDEN // 128, tile, 0)

        def down(n, _):
            n0 = pl.multiple_of(n * 256, 256)
            w = gvd[pl.ds(n * 4, 4), 2].reshape(256, HIDDEN)
            store(
                n0,
                lax.dot_general(hid[...], w, (((1,), (1,)), ((), ())), preferred_element_type=F32),
            )
            return 0

        lax.fori_loop(0, WIDTH // 256, down, 0)

    def keep(slot):
        def store(n0, value):
            sbuf[slot, :, pl.ds(n0, 256)] = value.astype(BF16)

        return store

    def add(slot, r0, ref):
        def body(n, _):
            n0 = pl.multiple_of(n * 256, 256)
            sbuf[slot, pl.ds(r0, 96), pl.ds(n0, 256)] = (
                sbuf[slot, pl.ds(r0, 96), pl.ds(n0, 256)].astype(F32) + ref[:, pl.ds(n0, 256)].astype(F32)
            ).astype(BF16)
            return 0

        lax.fori_loop(0, 8, body, 0)

    def top(ref):
        return ref.at[pl.ds(0, 96)]

    def bottom(ref):
        return ref.at[pl.ds(96, 96)]

    feed((x + 2) % 4, keep(0))
    qa = remote(top(sbuf.at[0]), ra, qsend.at[0], qrecv.at[0], dev_x(1))
    qb = remote(bottom(sbuf.at[0]), rb, qsend.at[1], qrecv.at[1], dev_x(-1))
    start(qa)
    start(qb)
    feed((x + 1) % 4, keep(1))
    q2 = remote(bottom(sbuf.at[1]), bottom(rl), qsend.at[2], qrecv.at[2], dev_x(1))
    start(q2)
    qa.wait_recv()
    add(1, 0, ra)
    q3 = remote(top(sbuf.at[1]), top(rl), qsend.at[3], qrecv.at[3], dev_x(1))
    start(q3)
    feed((x + 3) % 4, keep(2))
    q4 = remote(top(sbuf.at[2]), top(rr), qsend.at[4], qrecv.at[4], dev_x(-1))
    start(q4)
    qb.wait_recv()
    add(2, 96, rb)
    q5 = remote(bottom(sbuf.at[2]), bottom(rr), qsend.at[5], qrecv.at[5], dev_x(-1))
    start(q5)

    def hold(n0, value):
        own[:, pl.ds(n0, 256)] = value

    feed(x, hold)
    x0 = pl.multiple_of(x * SHARE, 64)
    q2.wait_recv()
    q3.wait_recv()
    q4.wait_recv()
    q5.wait_recv()

    def finish(n, _):
        n0 = pl.multiple_of(n * 256, 256)
        cols = pl.ds(n0, 256)
        out[:, cols] = (
            stream[pl.ds(x0, SHARE), cols].astype(F32)
            + own[:, cols]
            + rl[:, cols].astype(F32)
            + rr[:, cols].astype(F32)
        ).astype(BF16)
        return 0

    lax.fori_loop(0, 8, finish, 0)

    for copy in pending:
        copy.wait_send()
    for i in range(BLOCKS):
        ag_right(i).wait_send()
        ag_left(i).wait_send()
        ag_forward_right(i).wait_send()
        ag_forward_left(i).wait_send()

    @pl.when(sp < 31)
    def _():
        for h in halo:
            h.wait_send()
        rim.wait_send()


def on_device(
    mixer_value_projection,
    write_vectors_projected,
    read_vectors_projected,
    output_gate_projected,
    step_size_scores,
    position_decay_extra,
    step_size_bias,
    head_decay_logarithm,
    value_filter_taps,
    write_filter_taps,
    read_filter_taps,
    gated_group_norm_gain,
    mixer_output_weight,
    residual,
    feedforward_norm_gain,
    feedforward_gate_weight,
    feedforward_value_weight,
    gate_filter_taps,
    single_value_filter_taps,
    feedforward_down_weight,
):
    args = (
        mixer_value_projection,
        write_vectors_projected.T,
        read_vectors_projected.T,
        output_gate_projected,
        step_size_scores.T,
        position_decay_extra.T,
        step_size_bias,
        head_decay_logarithm,
        value_filter_taps,
        jnp.concatenate([write_filter_taps, read_filter_taps], axis=1).T,
        gated_group_norm_gain.reshape(1, INNER),
        mixer_output_weight.reshape(32, 16, WIDTH),
        residual,
        feedforward_norm_gain.reshape(1, WIDTH),
        feedforward_gate_weight,
        feedforward_value_weight,
        gate_filter_taps,
        single_value_filter_taps,
        feedforward_down_weight.T,
    )
    hbm = pl.BlockSpec(memory_space=pl.ANY)
    vmem = pl.BlockSpec(memory_space=pltpu.VMEM)
    smem = pl.BlockSpec(memory_space=pltpu.SMEM)
    specs = [hbm, hbm, hbm, hbm, vmem, vmem, smem, smem, vmem, vmem, vmem, hbm, hbm, vmem, hbm, hbm, vmem, vmem, hbm]
    dma = pltpu.SemaphoreType.DMA
    scratch = [
        pltpu.VMEM((16 + ROWS, INNER), BF16),
        pltpu.VMEM((128, 128 + ROWS), BF16),
        pltpu.VMEM((ROWS, INNER), BF16),
        pltpu.VMEM((BLOCKS, HEADS, BLOCK), F32),
        pltpu.VMEM((BLOCKS, HEADS, BLOCK), F32),
        pltpu.VMEM((BLOCKS, 64, BLOCK), BF16),
        pltpu.VMEM((BLOCKS, BLOCK, 64), BF16),
        pltpu.VMEM((ROWS, INNER), BF16),
        pltpu.VMEM((ROWS, INNER), F32),
        pltpu.VMEM((ROWS, INNER), F32),
        pltpu.VMEM((BLOCKS, 64, INNER), F32),
        pltpu.VMEM((BLOCKS, 1, INNER), F32),
        pltpu.VMEM((64, INNER), F32),
        pltpu.VMEM((1, INNER), F32),
        pltpu.VMEM((96, INNER), BF16),
        pltpu.VMEM((96, INNER), BF16),
        pltpu.VMEM((4, 96, INNER), BF16),
        pltpu.VMEM((4, 96, INNER), BF16),
        pltpu.VMEM((2, 64, INNER), F32),
        pltpu.VMEM((4, ROWS, INNER), BF16),
        pltpu.VMEM((ROWS, WIDTH), BF16),
        pltpu.VMEM((16 + ROWS, WIDTH), BF16),
        pltpu.VMEM((4, 32, 16, WIDTH), BF16),
        pltpu.VMEM((32, 3, 64, HIDDEN), BF16),
        pltpu.VMEM((SHARE, HIDDEN), BF16),
        pltpu.VMEM((3, SHARE, WIDTH), BF16),
        pltpu.VMEM((96, WIDTH), BF16),
        pltpu.VMEM((96, WIDTH), BF16),
        pltpu.VMEM((SHARE, WIDTH), BF16),
        pltpu.VMEM((SHARE, WIDTH), BF16),
        pltpu.VMEM((SHARE, WIDTH), F32),
        dma((9,)),
        dma((4,)),
        dma((4,)),
        dma((3,)),
        dma((3,)),
        dma((7,)),
        dma((7,)),
        dma((3, 36)),
        dma((3, 36)),
        dma((4, BLOCKS)),
        dma((4, BLOCKS)),
        dma((6,)),
        dma((6,)),
    ]
    return pl.pallas_call(
        kernel,
        out_shape=jax.ShapeDtypeStruct((SHARE, WIDTH), BF16),
        in_specs=specs,
        out_specs=vmem,
        scratch_shapes=scratch,
        compiler_params=pltpu.CompilerParams(
            collective_id=0, has_side_effects=True, vmem_limit_bytes=64 * 1024 * 1024 - 65536
        ),
        name="layer",
    )(*args)


def solution(mesh):
    torus = Mesh(mesh.devices.reshape(4, 4, 2, mesh.shape["tp"]), ("sp_0", "sp_1", "sp_2", "tp"))
    in_specs = (
        P(SP, "tp"),
        P(SP, "tp"),
        P(SP, "tp"),
        P(SP, "tp"),
        P(SP, "tp"),
        P(SP, "tp"),
        P("tp"),
        P("tp"),
        P(None, "tp"),
        P(None, "tp"),
        P(None, "tp"),
        P("tp"),
        P("tp", None),
        P(SP, None),
        P(),
        P(SP, "tp"),
        P(SP, "tp"),
        P(None, "tp"),
        P(None, "tp"),
        P("tp", SP),
    )
    return jax.shard_map(
        on_device, mesh=torus, in_specs=in_specs, out_specs=P(SP_TP, None), check_vma=False
    )
```

```python
import functools

import jax
import jax.numpy as jnp
from jax import lax
from jax.experimental import pallas as pl
from jax.experimental.pallas import tpu as pltpu
from jax.sharding import Mesh
from jax.sharding import PartitionSpec as P

SP = ("sp_0", "sp_1", "sp_2")
SP_TP = ("sp_0", "sp_1", "sp_2", "tp")
MESH = pl.DeviceIdType.MESH
EPS = 1e-06
F32 = jnp.float32
BF16 = jnp.bfloat16
HI = lax.Precision.HIGHEST

ROWS = 768
BLOCK = 128
BLOCKS = 6
HEADS = 8
INNER = 512
WIDTH = 2048
HIDDEN = 1408
SHARE = 192
PLANE = 1024


def silu(v):
    return v / (1.0 + jnp.exp(-v))


def dot(a, b):
    return jnp.dot(a, b, preferred_element_type=F32)


def kernel(
    xv, wrt, rdt, og, sct, ext, bias, hlog, vtap, wtap, rtap, ggain, wout, res, fgain, gw, vw, gtap, vtap2, dwt,
    out,
    xs, bct, ogs, st_s, cum_s, bt_s, c_s, sc_s, ecx_s, ins_s, lb_s, pre_s, stv, plog,
    m1, r1, r2, r3, exc, inc,
    ng, stream, fin, wof, gvd, rows, hid, sbuf, ra, rb, rl, rr, own,
    lsem, vsend, vrecv, hsend, hrecv, xsend, xrecv, ssend, srecv, wsend, wrecv, asend, arecv, qsend, qrecv,
):
    z = lax.axis_index("sp_0")
    y = lax.axis_index("sp_1")
    c = lax.axis_index("sp_2")
    x = lax.axis_index("tp")
    sp = z * 8 + y * 2 + c

    def at_sp(s):
        return ((s // 8) % 4, (s // 2) % 4, s % 2, x)

    nxt = at_sp(sp + 1)
    prv = at_sp(sp + 31)
    partner = (z, y, 1 - c, x)

    def dev_x(d):
        return (z, y, c, (x + d + 4) % 4)

    def dev_y(d):
        return (z, (y + d) % 4, c, x)

    def dev_z(d):
        return ((z + d) % 4, y, c, x)

    def dev1(d):
        return ((z + 4 + d * c) % 4, (y + 4 + d * (1 - c)) % 4, c, x)

    def dev2(d):
        return ((z + 4 + d * (1 - c)) % 4, (y + 4 + d * c) % 4, c, x)

    ca = c * z + (1 - c) * y
    cb = c * y + (1 - c) * z

    def item(da, db):
        return ((ca + 4 + da) % 4) * (2 + 6 * c) + ((cb + 4 + db) % 4) * (8 - 6 * c) + c

    def remote(src, dst, ss, rs, dev):
        return pltpu.make_async_remote_copy(
            src_ref=src, dst_ref=dst, send_sem=ss, recv_sem=rs, device_id=dev, device_id_type=MESH
        )

    loads = [
        pltpu.make_async_copy(xv, xs.at[pl.ds(16, ROWS)], lsem.at[0]),
        pltpu.make_async_copy(wrt, bct.at[pl.ds(0, 64), pl.ds(128, ROWS)], lsem.at[1]),
        pltpu.make_async_copy(rdt, bct.at[pl.ds(64, 64), pl.ds(128, ROWS)], lsem.at[2]),
        pltpu.make_async_copy(gw, gvd.at[sp, 0], lsem.at[3]),
        pltpu.make_async_copy(vw, gvd.at[sp, 1], lsem.at[4]),
        pltpu.make_async_copy(dwt, gvd.at[sp, 2], lsem.at[5]),
        pltpu.make_async_copy(og, ogs, lsem.at[6]),
        pltpu.make_async_copy(wout, wof.at[0], lsem.at[7]),
        pltpu.make_async_copy(res, stream, lsem.at[8]),
    ]
    for load in loads:
        load.start()

    barrier = pltpu.get_barrier_semaphore()
    peers = [partner, nxt, prv]
    for d in (1, 2, 3):
        peers += [dev_x(d), dev_y(d), dev_z(d)]
    for peer in peers:
        pl.semaphore_signal(barrier, inc=1, device_id=peer, device_id_type=MESH)

    pending = []

    def start(copy):
        copy.start()
        pending.append(copy)

    halo = [
        remote(xv.at[pl.ds(ROWS - 16, 16)], xs.at[pl.ds(0, 16)], hsend.at[0], hrecv.at[0], nxt),
        remote(wrt.at[:, pl.ds(ROWS - 128, 128)], bct.at[pl.ds(0, 64), pl.ds(0, 128)], hsend.at[1], hrecv.at[1], nxt),
        remote(rdt.at[:, pl.ds(ROWS - 128, 128)], bct.at[pl.ds(64, 64), pl.ds(0, 128)], hsend.at[2], hrecv.at[2], nxt),
    ]

    @pl.when(sp == 0)
    def _():
        xs[pl.ds(0, 16), :] = jnp.zeros((16, INNER), BF16)
        bct[:, pl.ds(0, 128)] = jnp.zeros((128, 128), BF16)
        fin[pl.ds(0, 16), :] = jnp.zeros((16, WIDTH), BF16)

    def piece(r):
        return remote(
            wout.at[sp, :, pl.ds(0, PLANE)],
            wof.at[r, sp, :, pl.ds(0, PLANE)],
            xsend.at[r - 1],
            xrecv.at[r - 1],
            dev_x(-r),
        )

    def full(batch, k):
        if batch == 0:
            return wof.at[pl.ds(1, 3), k, :, pl.ds(0, PLANE)]
        if batch == 1:
            return gvd.at[k, pl.ds(0, 2)]
        return gvd.at[k, 2]

    def half(batch, k, side):
        if batch == 0:
            return wof.at[pl.ds(1, 3), k, :, pl.ds(PLANE // 2 * side, PLANE // 2)]
        if batch == 1:
            return gvd.at[k, side]
        return gvd.at[k, 2, pl.ds(32 * side, 32)]

    right = pl.ds(PLANE, WIDTH - PLANE)

    def slab(r, core):
        return wof.at[r, pl.ds(pl.multiple_of(16 * core, 16), 16), :, right]

    def slab_half(r, core, side):
        return wof.at[r, pl.ds(pl.multiple_of(16 * core + 8 * side, 8), 8), :, right]

    own_slab = wout.at[pl.ds(pl.multiple_of(16 * c, 16), 16), :, right]
    w_right = remote(own_slab, slab(3, c), vsend.at[0], vrecv.at[0], dev_x(1))
    w_left = remote(own_slab, slab(1, c), vsend.at[1], vrecv.at[1], dev_x(-1))
    w_fright = remote(slab_half(3, c, 0), slab_half(2, c, 0), vsend.at[2], vrecv.at[2], dev_x(1))
    w_fleft = remote(slab_half(1, c, 1), slab_half(2, c, 1), vsend.at[3], vrecv.at[3], dev_x(-1))

    def slab_partner(r):
        return remote(slab(r, c), slab(r, c), vsend.at[3 + r], vrecv.at[3 + r], partner)

    def slab_events():
        w_right.wait_recv()
        start(w_fright)
        start(slab_partner(3))
        w_left.wait_recv()
        start(w_fleft)
        start(slab_partner(1))

    def slab_last():
        w_fright.wait_recv()
        w_fleft.wait_recv()
        start(slab_partner(2))

    def slab_from_partner():
        for r in (1, 2, 3):
            remote(
                slab(r, 1 - c), slab(r, 1 - c), vsend.at[3 + r], vrecv.at[3 + r], partner
            ).wait_recv()

    def send(batch, ref, sem, dev):
        start(remote(ref, ref, wsend.at[batch, sem], wrecv.at[batch, sem], dev))

    def arrive(batch, ref, sem):
        remote(ref, ref, wsend.at[batch, sem], wrecv.at[batch, sem], partner).wait_recv()

    def to_partner(batch, k):
        ref = full(batch, k)
        start(remote(ref, ref, wsend.at[batch, 20 + k // 2], wrecv.at[batch, 20 + k // 2], partner))

    order = (0, -1, 1, 2)

    def first_sends(batch):
        k = item(0, 0)
        send(batch, full(batch, k), 1, dev1(-1))
        send(batch, full(batch, k), 0, dev1(1))

    def second_copies(batch, j):
        ref = full(batch, item(order[j], 0))
        copies = [
            remote(ref, ref, wsend.at[batch, 5 + 4 * j], wrecv.at[batch, 5 + 4 * j], dev2(-1)),
            remote(ref, ref, wsend.at[batch, 4 + 4 * j], wrecv.at[batch, 4 + 4 * j], dev2(1)),
        ]
        pending.extend(copies)
        return copies

    def second_sends(batch, j):
        for copy in second_copies(batch, j):
            copy.start()
        to_partner(batch, item(order[j], 0))

    def first_copies(batch):
        k = item(-1, 0)
        k2 = item(1, 0)
        ref, ref2 = half(batch, k, 0), half(batch, k2, 1)
        copies = [
            remote(ref, ref, wsend.at[batch, 2], wrecv.at[batch, 2], dev1(1)),
            remote(ref2, ref2, wsend.at[batch, 3], wrecv.at[batch, 3], dev1(-1)),
        ]
        pending.extend(copies)
        return copies

    def first_forward(batch, copies):
        arrive(batch, full(batch, item(-1, 0)), 0)
        copies[0].start()
        arrive(batch, full(batch, item(1, 0)), 1)
        copies[1].start()

    def third_event(batch):
        k = item(2, 0)
        arrive(batch, half(batch, k, 0), 2)
        arrive(batch, half(batch, k, 1), 3)
        second_sends(batch, 3)

    def second_events(batch, j):
        base = 4 + 4 * j
        k = item(order[j], -1)
        arrive(batch, full(batch, k), base)
        send(batch, half(batch, k, 0), base + 2, dev2(1))
        to_partner(batch, k)
        k = item(order[j], 1)
        arrive(batch, full(batch, k), base + 1)
        send(batch, half(batch, k, 1), base + 3, dev2(-1))
        to_partner(batch, k)

    def last_events(batch, j):
        base = 4 + 4 * j
        k = item(order[j], 2)
        arrive(batch, half(batch, k, 0), base + 2)
        arrive(batch, half(batch, k, 1), base + 3)
        to_partner(batch, k)

    def from_partner(batch):
        for i in range(16):
            arrive(batch, full(batch, 2 * i + 1 - c), 20 + i)

    head = lax.broadcasted_iota(jnp.int32, (HEADS, 1), 0)
    bias_c = jnp.zeros((HEADS, 1), F32)
    rate_c = jnp.zeros((HEADS, 1), F32)
    for h in range(HEADS):
        bias_c = jnp.where(head == h, bias[h], bias_c)
        rate_c = jnp.where(head == h, hlog[h], rate_c)
    rate_c = jnp.exp(rate_c)
    v = sct[...] + bias_c
    step = jnp.maximum(v, 0.0) + jnp.log1p(jnp.exp(-jnp.abs(v)))
    logd = -step * rate_c + ext[...]
    row_i = lax.broadcasted_iota(jnp.int32, (BLOCK, BLOCK), 0)
    col_i = lax.broadcasted_iota(jnp.int32, (BLOCK, BLOCK), 1)
    upper = (row_i <= col_i).astype(F32)
    for b in range(BLOCKS):
        st_s[b] = step[:, b * BLOCK : (b + 1) * BLOCK]
        cum_s[b] = jnp.dot(
            logd[:, b * BLOCK : (b + 1) * BLOCK], upper, preferred_element_type=F32, precision=HI
        )

    def expand(value):
        spread = (
            lax.broadcasted_iota(jnp.int32, (HEADS, INNER), 1) // 64
            == lax.broadcasted_iota(jnp.int32, (HEADS, INNER), 0)
        ).astype(F32)
        return jnp.dot(value.T, spread, preferred_element_type=F32, precision=HI)

    loads[0].wait()
    loads[1].wait()
    loads[2].wait()
    vt = vtap[...].astype(F32)
    bt = jnp.concatenate([wtap[...].astype(F32).T, rtap[...].astype(F32).T], axis=0)

    def local(b, _):
        r0 = pl.multiple_of(b * BLOCK, BLOCK)
        vals = xs[pl.ds(r0, BLOCK + 16), :].astype(F32)
        conv = vt[3:4] * vals
        for j in range(3):
            conv = conv + vt[j : j + 1] * pltpu.roll(vals, 3 - j, 0)
        xc = silu(conv[16:]).astype(BF16).astype(F32)
        lanes = bct[:, pl.ds(r0, 2 * BLOCK)].astype(F32)
        conv2 = bt[:, 3:4] * lanes
        for j in range(3):
            conv2 = conv2 + bt[:, j : j + 1] * pltpu.roll(lanes, 3 - j, 1)
        bc = silu(conv2[:, BLOCK:])
        wt = bc[:64].astype(BF16)
        rd = bc[64:].T.astype(BF16)
        bt_s[b] = wt
        c_s[b] = rd
        cumx = expand(cum_s[b])
        stepx = expand(st_s[b])
        last = cumx[BLOCK - 1 : BLOCK]
        scaled = (xc * stepx).astype(BF16)
        sc_s[pl.ds(r0, BLOCK), :] = scaled
        tailed = (scaled.astype(F32) * jnp.exp(last - cumx)).astype(BF16)
        ecx_s[pl.ds(r0, BLOCK), :] = jnp.exp(cumx)
        fresh = dot(wt, tailed)
        lb_s[b] = fresh
        pre_s[b] = last
        return 0

    def inner(b, _):
        r0 = pl.multiple_of(b * BLOCK, BLOCK)
        s = dot(c_s[b], bt_s[b])
        cum = cum_s[b]
        cumt = cum.T
        causal = (
            lax.broadcasted_iota(jnp.int32, (BLOCK, BLOCK), 0)
            >= lax.broadcasted_iota(jnp.int32, (BLOCK, BLOCK), 1)
        )
        low = lax.broadcasted_iota(jnp.int32, (BLOCK, BLOCK), 1) < 64
        for p in range(HEADS // 2):
            rhs = sc_s[pl.ds(r0, BLOCK), pl.ds(p * 128, 128)]
            parts = []
            for h in (2 * p, 2 * p + 1):
                spread = jnp.where(causal, cumt[:, h : h + 1] - cum[h : h + 1, :], -jnp.inf)
                parts.append(dot((s * jnp.exp(spread)).astype(BF16), rhs))
            ins_s[pl.ds(r0, BLOCK), pl.ds(p * 128, 128)] = jnp.where(low, parts[0], parts[1])
        return 0

    def put(ref, decay, state):
        ref[pl.ds(0, 64), :] = state.astype(BF16)
        d = jnp.broadcast_to(decay, (16, decay.shape[1]))
        high = d.astype(BF16)
        ref[pl.ds(64, 16), :] = high
        ref[pl.ds(80, 16), :] = (d - high.astype(F32)).astype(BF16)

    def take(ref, cols=slice(None)):
        decay = ref[pl.ds(64, 16), cols].astype(F32) + ref[pl.ds(80, 16), cols].astype(F32)
        return decay[0:1], ref[pl.ds(0, 64), cols].astype(F32)

    def wait_pieces():
        for r in (1, 2, 3):
            piece(r).wait_recv()

    lax.fori_loop(1, 3, local, 0)
    pl.semaphore_wait(barrier, len(peers))

    @pl.when(sp < 31)
    def _():
        for h in halo:
            h.start()

    for r in (1, 2, 3):
        start(piece(r))
    start(w_right)
    start(w_left)
    for i in (3, 4, 5):
        loads[i].wait()
    for batch in (1, 2):
        k = item(0, 0)
        send(batch, full(batch, k), 1, dev1(-1))
        send(batch, full(batch, k), 0, dev1(1))
    lax.fori_loop(3, BLOCKS, local, 0)

    @pl.when(sp > 0)
    def _():
        for h in halo:
            h.wait_recv()

    lax.fori_loop(0, 1, local, 0)
    state = jnp.zeros((64, INNER), F32)
    total_log = jnp.zeros((1, INNER), F32)
    for b in range(BLOCKS):
        fresh, last = lb_s[b], pre_s[b]
        lb_s[b] = state
        pre_s[b] = total_log
        state = state * jnp.exp(last) + fresh
        total_log = total_log + last
    stv[...] = state
    plog[...] = total_log
    put(m1, jnp.exp(total_log), state)
    wait_pieces()
    first_sends(0)
    q0 = remote(m1, r1, ssend.at[0], srecv.at[0], partner)
    start(q0)
    lax.fori_loop(0, 3, inner, 0)
    q0.wait_recv()

    mine = pl.ds(pl.multiple_of(c * 256, 256), 256)
    d_own, s_own = jnp.exp(plog[:, mine]), stv[:, mine]
    d_par, s_par = take(r1, mine)
    is_first = c == 0
    chip_s = jnp.where(is_first, s_own * d_par + s_par, s_par * d_own + s_own)
    put(r2.at[y], d_own * d_par, chip_s)
    for d in (1, 2, 3):
        start(remote(r2.at[y], r2.at[y], ssend.at[d], srecv.at[d], dev_y(d)))
    early = second_copies(1, 0)
    forwards = [first_copies(batch) for batch in range(3)]

    @pl.when(c == 0)
    def _():
        for copy in early:
            copy.start()

    @pl.when(c == 1)
    def _():
        for batch in range(3):
            first_forward(batch, forwards[batch])

    lax.fori_loop(3, BLOCKS, inner, 0)
    for d in (1, 2, 3):
        src = (y + 4 - d) % 4
        remote(r2.at[src], r2.at[src], ssend.at[d], srecv.at[d], dev_y(d)).wait_recv()
    row_d, row_s = take(r2.at[0])
    exc_d = jnp.where(y > 0, row_d, 1.0)
    exc_s = jnp.where(y > 0, row_s, 0.0)
    for i in (1, 2, 3):
        di, si = take(r2.at[i])
        row_s = row_s * di + si
        row_d = row_d * di
        exc_s = jnp.where(y > i, exc_s * di + si, exc_s)
        exc_d = jnp.where(y > i, exc_d * di, exc_d)
    put(r3.at[z], row_d, row_s)
    exc[0] = exc_s
    exc[1] = jnp.broadcast_to(exc_d, (64, 256))
    for d in (1, 2, 3):
        start(remote(r3.at[z], r3.at[z], ssend.at[3 + d], srecv.at[3 + d], dev_z(d)))

    @pl.when(c == 1)
    def _():
        for copy in early:
            copy.start()

    @pl.when(c == 0)
    def _():
        for batch in range(3):
            first_forward(batch, forwards[batch])

    slab_events()
    for d in (1, 2, 3):
        src = (z + 4 - d) % 4
        remote(r3.at[src], r3.at[src], ssend.at[3 + d], srecv.at[3 + d], dev_z(d)).wait_recv()
    acc = jnp.zeros((64, 256), F32)
    for i in (0, 1, 2):
        di, si = take(r3.at[i])
        acc = jnp.where(z > i, acc * di + si, acc)
    inc[c] = acc * exc[1] + exc[0]
    q1 = remote(inc.at[c], inc.at[c], ssend.at[7], srecv.at[7], partner)
    start(q1)
    for j in (0, 1, 2):
        second_sends(0, j)
    remote(inc.at[1 - c], inc.at[1 - c], ssend.at[7], srecv.at[7], partner).wait_recv()
    d_par, s_par = take(r1)
    arrived = jnp.concatenate([inc[0], inc[1]], axis=1)
    stv[...] = jnp.where(is_first, arrived, arrived * d_par + s_par)

    loads[6].wait()
    gain = ggain[...]

    def block_of(i):
        return (i + 4) % 6

    def rows_of(i):
        return pl.multiple_of(block_of(i) * BLOCK, BLOCK)

    def ng_full(r, i):
        return ng.at[r, pl.ds(rows_of(i), BLOCK)]

    def ng_half(r, i, side):
        return ng.at[r, pl.ds(pl.multiple_of(rows_of(i) + 64 * side, 64), 64)]

    def ag_right(i):
        return remote(ng_full(0, i), ng_full(3, i), asend.at[0, i], arecv.at[0, i], dev_x(1))

    def ag_left(i):
        return remote(ng_full(0, i), ng_full(1, i), asend.at[1, i], arecv.at[1, i], dev_x(-1))

    def ag_forward_right(i):
        return remote(ng_half(3, i, 0), ng_half(2, i, 0), asend.at[2, i], arecv.at[2, i], dev_x(1))

    def ag_forward_left(i):
        return remote(ng_half(1, i, 1), ng_half(2, i, 1), asend.at[3, i], arecv.at[3, i], dev_x(-1))

    def final(i, _):
        b = block_of(i)
        r0 = rows_of(i)
        state = lb_s[b] + stv[...] * jnp.exp(pre_s[b])
        ent = dot(c_s[b], state.astype(BF16))
        m = ins_s[pl.ds(r0, BLOCK), :] + ecx_s[pl.ds(r0, BLOCK), :] * ent
        g = m * silu(ogs[pl.ds(r0, BLOCK), :].astype(F32))
        scale = lax.rsqrt(jnp.mean(g * g, axis=-1, keepdims=True) + EPS)
        ng[0, pl.ds(r0, BLOCK), :] = (g * scale * gain).astype(BF16)

        @pl.when((i > 0) & (i < 5))
        def _():
            ag_right(i - 1).start()
            ag_left(i - 1).start()

        return 0

    lax.fori_loop(0, BLOCKS, final, 0)
    third_event(0)

    def ag_forward(i):
        ag_right(i).wait_recv()
        ag_forward_right(i).start()
        ag_left(i).wait_recv()
        ag_forward_left(i).start()

    def ag_last(i):
        ag_forward_right(i).wait_recv()
        ag_forward_left(i).wait_recv()

    to_partner(1, item(0, 0))
    second_sends(1, 1)
    slab_last()
    ag_forward(0)
    ag_right(4).start()
    ag_left(4).start()
    for j in range(4):
        second_events(0, j)
    second_sends(1, 2)
    third_event(1)
    ag_forward(1)
    ag_right(5).start()
    ag_left(5).start()
    ag_forward(2)
    for j in range(4):
        last_events(0, j)
    second_sends(2, 0)
    second_sends(2, 1)
    second_sends(2, 2)
    third_event(2)
    second_events(1, 0)
    ag_forward(3)
    loads[7].wait()
    loads[8].wait()

    def project(g):
        ag_last(2 * g)
        ag_last(2 * g + 1)
        r0 = ((g + 2) % 3) * 256

        def tile(n, total):
            n0 = pl.multiple_of(n * 512, 512)
            part = dot(ng[0, pl.ds(r0, 256), :], wof[0, :, :, pl.ds(n0, 512)].reshape(INNER, 512))
            for r in (1, 2, 3):
                part = part + dot(
                    ng[r, pl.ds(r0, 256), :], wof[r, :, :, pl.ds(n0, 512)].reshape(INNER, 512)
                )
            s = (stream[pl.ds(r0, 256), pl.ds(n0, 512)].astype(F32) + part).astype(BF16)
            stream[pl.ds(r0, 256), pl.ds(n0, 512)] = s
            sf = s.astype(F32)
            return total + jnp.sum(sf * sf, axis=-1, keepdims=True)

        total = lax.fori_loop(0, 4, tile, jnp.zeros((256, 1), F32), unroll=True)
        scale = lax.rsqrt(total * (1.0 / WIDTH) + EPS)

        def norm(n, _):
            n0 = pl.multiple_of(n * 256, 256)
            sf = stream[pl.ds(r0, 256), pl.ds(n0, 256)].astype(F32)
            fin[pl.ds(16 + r0, 256), pl.ds(n0, 256)] = (
                sf * scale * fgain[:, pl.ds(n0, 256)]
            ).astype(BF16)
            return 0

        lax.fori_loop(0, 8, norm, 0)

    slab_from_partner()
    from_partner(0)
    second_events(1, 1)
    project(0)
    rim = remote(fin.at[pl.ds(ROWS, 16)], fin.at[pl.ds(0, 16)], hsend.at[3], hrecv.at[3], nxt)

    @pl.when(sp < 31)
    def _():
        rim.start()

    ag_forward(4)
    second_events(1, 2)
    ag_forward(5)
    second_events(1, 3)
    last_events(1, 0)
    project(1)
    last_events(1, 1)
    second_events(2, 0)
    second_events(2, 1)
    last_events(1, 2)
    project(2)
    second_events(2, 2)
    second_events(2, 3)
    last_events(1, 3)

    @pl.when(sp > 0)
    def _():
        rim.wait_recv()

    from_partner(1)

    def gates(segments):
        at = [pl.multiple_of(d * SHARE + 96 * side, 32) for d, side in segments]

        def product(n, slot):
            n0 = pl.multiple_of(n * 128, 128)
            w = jnp.concatenate(
                [
                    gvd[:, 0, :, pl.ds(n0, 128)].reshape(WIDTH, 128),
                    gvd[:, 1, :, pl.ds(n0, 128)].reshape(WIDTH, 128),
                ],
                axis=1,
            )
            both = jnp.concatenate([fin[pl.ds(f0, 112), :] for f0 in at], axis=0)
            rows[slot] = dot(both, w).astype(BF16)

        def gate(n, slot):
            n0 = pl.multiple_of(n * 128, 128)
            u = rows[slot].astype(F32)
            taps = jnp.concatenate(
                [gtap[:, pl.ds(n0, 128)].astype(F32), vtap2[:, pl.ds(n0, 128)].astype(F32)], axis=1
            )
            conv = taps[2:3] * u
            for j in range(2):
                conv = conv + taps[j : j + 1] * pltpu.roll(u, 2 - j, 0)
            conv = jnp.concatenate([conv[16:112], conv[128:]], axis=0)
            hid[:, pl.ds(n0, 128)] = (silu(conv[:, :128]) * conv[:, 128:]).astype(BF16)

        def tile(i, _):
            gate(2 * i, 0)
            gate(2 * i + 1, 1)
            product(2 * i + 2, 0)
            product(2 * i + 3, 1)
            return 0

        product(0, 0)
        product(1, 1)
        lax.fori_loop(0, 4, tile, 0)
        gate(8, 0)
        gate(9, 1)
        product(10, 0)
        gate(10, 0)

    def downs(first, end, store):
        def down(n, _):
            n0 = pl.multiple_of(n * 512, 512)
            w = gvd[pl.ds(n * 8, 8), 2].reshape(512, HIDDEN)
            store(
                n0,
                lax.dot_general(hid[...], w, (((1,), (1,)), ((), ())), preferred_element_type=F32),
            )
            return 0

        lax.fori_loop(first, end, down, 0, unroll=True)

    def feed(segments, store):
        gates(segments)
        downs(0, 4, store)

    def keep(slot):
        def store(n0, value):
            sbuf[slot, :, pl.ds(n0, 512)] = value.astype(BF16)

        return store

    def add(slot, r0, ref):
        def body(n, _):
            n0 = pl.multiple_of(n * 256, 256)
            sbuf[slot, pl.ds(r0, 96), pl.ds(n0, 256)] = (
                sbuf[slot, pl.ds(r0, 96), pl.ds(n0, 256)].astype(F32) + ref[:, pl.ds(n0, 256)].astype(F32)
            ).astype(BF16)
            return 0

        lax.fori_loop(0, 8, body, 0)

    def top(ref):
        return ref.at[pl.ds(0, 96)]

    def bottom(ref):
        return ref.at[pl.ds(96, 96)]

    gates([((x + 2) % 4, 0), ((x + 2) % 4, 1)])
    for j in range(4):
        last_events(2, j)
    from_partner(2)
    firsts = []
    for i in (0, 1):
        cols = pl.ds(1024 * i, 1024)
        downs(2 * i, 2 * i + 2, keep(0))
        qa = remote(
            sbuf.at[0, pl.ds(0, 96), cols], ra.at[:, cols], qsend.at[2 * i], qrecv.at[2 * i], dev_x(1)
        )
        qb = remote(
            sbuf.at[0, pl.ds(96, 96), cols], rb.at[:, cols], qsend.at[2 * i + 1], qrecv.at[2 * i + 1], dev_x(-1)
        )
        start(qa)
        start(qb)
        firsts.append((qa, qb))
    feed([((x + 1) % 4, 1), ((x + 3) % 4, 0)], keep(1))
    q2 = remote(top(sbuf.at[1]), bottom(rl), qsend.at[4], qrecv.at[4], dev_x(1))
    q4 = remote(bottom(sbuf.at[1]), top(rr), qsend.at[5], qrecv.at[5], dev_x(-1))
    start(q2)
    start(q4)
    feed([((x + 1) % 4, 0), ((x + 3) % 4, 1)], keep(2))
    for qa, _ in firsts:
        qa.wait_recv()
    add(2, 0, ra)
    q3 = remote(top(sbuf.at[2]), top(rl), qsend.at[6], qrecv.at[6], dev_x(1))
    start(q3)
    for _, qb in firsts:
        qb.wait_recv()
    add(2, 96, rb)
    q5 = remote(bottom(sbuf.at[2]), bottom(rr), qsend.at[7], qrecv.at[7], dev_x(-1))
    start(q5)

    def hold(n0, value):
        own[:, pl.ds(n0, 512)] = value

    feed([(x, 0), (x, 1)], hold)
    x0 = pl.multiple_of(x * SHARE, 64)
    q2.wait_recv()
    q3.wait_recv()
    q4.wait_recv()
    q5.wait_recv()

    def finish(n, _):
        n0 = pl.multiple_of(n * 256, 256)
        cols = pl.ds(n0, 256)
        out[:, cols] = (
            stream[pl.ds(x0, SHARE), cols].astype(F32)
            + own[:, cols]
            + rl[:, cols].astype(F32)
            + rr[:, cols].astype(F32)
        ).astype(BF16)
        return 0

    lax.fori_loop(0, 8, finish, 0)

    for copy in pending:
        copy.wait_send()
    for i in range(BLOCKS):
        ag_right(i).wait_send()
        ag_left(i).wait_send()
        ag_forward_right(i).wait_send()
        ag_forward_left(i).wait_send()

    @pl.when(sp < 31)
    def _():
        for h in halo:
            h.wait_send()
        rim.wait_send()


def on_device(
    mixer_value_projection,
    write_vectors_projected,
    read_vectors_projected,
    output_gate_projected,
    step_size_scores,
    position_decay_extra,
    step_size_bias,
    head_decay_logarithm,
    value_filter_taps,
    write_filter_taps,
    read_filter_taps,
    gated_group_norm_gain,
    mixer_output_weight,
    residual,
    feedforward_norm_gain,
    feedforward_gate_weight,
    feedforward_value_weight,
    gate_filter_taps,
    single_value_filter_taps,
    feedforward_down_weight,
):
    args = (
        mixer_value_projection,
        write_vectors_projected.T,
        read_vectors_projected.T,
        output_gate_projected,
        step_size_scores.T,
        position_decay_extra.T,
        step_size_bias,
        head_decay_logarithm,
        value_filter_taps,
        write_filter_taps,
        read_filter_taps,
        gated_group_norm_gain.reshape(1, INNER),
        mixer_output_weight.reshape(32, 16, WIDTH),
        residual,
        feedforward_norm_gain.reshape(1, WIDTH),
        feedforward_gate_weight,
        feedforward_value_weight,
        gate_filter_taps,
        single_value_filter_taps,
        feedforward_down_weight.T,
    )
    hbm = pl.BlockSpec(memory_space=pl.ANY)
    vmem = pl.BlockSpec(memory_space=pltpu.VMEM)
    smem = pl.BlockSpec(memory_space=pltpu.SMEM)
    specs = [hbm, hbm, hbm, hbm, vmem, vmem, smem, smem, vmem, vmem, vmem, vmem, hbm, hbm, vmem, hbm, hbm, vmem, vmem, hbm]
    dma = pltpu.SemaphoreType.DMA
    scratch = [
        pltpu.VMEM((16 + ROWS, INNER), BF16),
        pltpu.VMEM((128, 128 + ROWS), BF16),
        pltpu.VMEM((ROWS, INNER), BF16),
        pltpu.VMEM((BLOCKS, HEADS, BLOCK), F32),
        pltpu.VMEM((BLOCKS, HEADS, BLOCK), F32),
        pltpu.VMEM((BLOCKS, 64, BLOCK), BF16),
        pltpu.VMEM((BLOCKS, BLOCK, 64), BF16),
        pltpu.VMEM((ROWS, INNER), BF16),
        pltpu.VMEM((ROWS, INNER), F32),
        pltpu.VMEM((ROWS, INNER), F32),
        pltpu.VMEM((BLOCKS, 64, INNER), F32),
        pltpu.VMEM((BLOCKS, 1, INNER), F32),
        pltpu.VMEM((64, INNER), F32),
        pltpu.VMEM((1, INNER), F32),
        pltpu.VMEM((96, INNER), BF16),
        pltpu.VMEM((96, INNER), BF16),
        pltpu.VMEM((4, 96, 256), BF16),
        pltpu.VMEM((4, 96, 256), BF16),
        pltpu.VMEM((2, 64, 256), F32),
        pltpu.VMEM((2, 64, 256), F32),
        pltpu.VMEM((4, ROWS, INNER), BF16),
        pltpu.VMEM((ROWS, WIDTH), BF16),
        pltpu.VMEM((16 + ROWS, WIDTH), BF16),
        pltpu.VMEM((4, 32, 16, WIDTH), BF16),
        pltpu.VMEM((32, 3, 64, HIDDEN), BF16),
        pltpu.VMEM((2, SHARE + 32, 256), BF16),
        pltpu.VMEM((SHARE, HIDDEN), BF16),
        pltpu.VMEM((3, SHARE, WIDTH), BF16),
        pltpu.VMEM((96, WIDTH), BF16),
        pltpu.VMEM((96, WIDTH), BF16),
        pltpu.VMEM((SHARE, WIDTH), BF16),
        pltpu.VMEM((SHARE, WIDTH), BF16),
        pltpu.VMEM((SHARE, WIDTH), F32),
        dma((9,)),
        dma((7,)),
        dma((7,)),
        dma((4,)),
        dma((4,)),
        dma((3,)),
        dma((3,)),
        dma((8,)),
        dma((8,)),
        dma((3, 36)),
        dma((3, 36)),
        dma((4, BLOCKS)),
        dma((4, BLOCKS)),
        dma((8,)),
        dma((8,)),
    ]
    return pl.pallas_call(
        kernel,
        out_shape=jax.ShapeDtypeStruct((SHARE, WIDTH), BF16),
        in_specs=specs,
        out_specs=vmem,
        scratch_shapes=scratch,
        compiler_params=pltpu.CompilerParams(
            collective_id=0, has_side_effects=True, vmem_limit_bytes=64 * 1024 * 1024 - 65536
        ),
        name="layer",
    )(*args)


def solution(mesh):
    torus = Mesh(mesh.devices.reshape(4, 4, 2, mesh.shape["tp"]), ("sp_0", "sp_1", "sp_2", "tp"))
    in_specs = (
        P(SP, "tp"),
        P(SP, "tp"),
        P(SP, "tp"),
        P(SP, "tp"),
        P(SP, "tp"),
        P(SP, "tp"),
        P("tp"),
        P("tp"),
        P(None, "tp"),
        P(None, "tp"),
        P(None, "tp"),
        P("tp"),
        P("tp", None),
        P(SP, None),
        P(),
        P(SP, "tp"),
        P(SP, "tp"),
        P(None, "tp"),
        P(None, "tp"),
        P("tp", SP),
    )
    return jax.shard_map(
        on_device, mesh=torus, in_specs=in_specs, out_specs=P(SP_TP, None), check_vma=False
    )
```

```python
import functools

import jax
import jax.numpy as jnp
from jax import lax
from jax.experimental import pallas as pl
from jax.experimental.pallas import tpu as pltpu
from jax.sharding import Mesh
from jax.sharding import PartitionSpec as P

SP = ("sp_0", "sp_1", "sp_2")
SP_TP = ("sp_0", "sp_1", "sp_2", "tp")
MESH = pl.DeviceIdType.MESH
EPS = 1e-06
F32 = jnp.float32
BF16 = jnp.bfloat16
HI = lax.Precision.HIGHEST

ROWS = 768
BLOCK = 128
BLOCKS = 6
HEADS = 8
INNER = 512
WIDTH = 2048
HIDDEN = 1408
SHARE = 192
PLANE = 1024


def silu(v):
    return v / (1.0 + jnp.exp(-v))


def dot(a, b):
    return jnp.dot(a, b, preferred_element_type=F32)


def kernel(
    xv, wrt, rdt, og, sct, ext, bias, hlog, vtap, wtap, rtap, ggain, wout, res, fgain, gw, vw, gtap, vtap2, dwt,
    out,
    xs, bct, ogs, st_s, cum_s, bt_s, c_s, sc_s, ecx_s, ins_s, lb_s, pre_s, stv, plog,
    m1, r1, r2, r3, exc, inc,
    ng, stream, fin, wof, gvd, rows, hid, sbuf, ra, rb, rl, rr, own,
    lsem, vsend, vrecv, hsend, hrecv, xsend, xrecv, ssend, srecv, wsend, wrecv, asend, arecv, qsend, qrecv,
):
    z = lax.axis_index("sp_0")
    y = lax.axis_index("sp_1")
    c = lax.axis_index("sp_2")
    x = lax.axis_index("tp")
    sp = z * 8 + y * 2 + c

    def at_sp(s):
        return ((s // 8) % 4, (s // 2) % 4, s % 2, x)

    nxt = at_sp(sp + 1)
    prv = at_sp(sp + 31)
    partner = (z, y, 1 - c, x)

    def dev_x(d):
        return (z, y, c, (x + d + 4) % 4)

    def dev_y(d):
        return (z, (y + d) % 4, c, x)

    def dev_z(d):
        return ((z + d) % 4, y, c, x)

    def dev1(d):
        return ((z + 4 + d * c) % 4, (y + 4 + d * (1 - c)) % 4, c, x)

    def dev2(d):
        return ((z + 4 + d * (1 - c)) % 4, (y + 4 + d * c) % 4, c, x)

    ca = c * z + (1 - c) * y
    cb = c * y + (1 - c) * z

    def item(da, db):
        return ((ca + 4 + da) % 4) * (2 + 6 * c) + ((cb + 4 + db) % 4) * (8 - 6 * c) + c

    def remote(src, dst, ss, rs, dev):
        return pltpu.make_async_remote_copy(
            src_ref=src, dst_ref=dst, send_sem=ss, recv_sem=rs, device_id=dev, device_id_type=MESH
        )

    loads = [
        pltpu.make_async_copy(xv, xs.at[pl.ds(16, ROWS)], lsem.at[0]),
        pltpu.make_async_copy(wrt, bct.at[pl.ds(0, 64), pl.ds(128, ROWS)], lsem.at[1]),
        pltpu.make_async_copy(rdt, bct.at[pl.ds(64, 64), pl.ds(128, ROWS)], lsem.at[2]),
        pltpu.make_async_copy(gw, gvd.at[sp, 0], lsem.at[3]),
        pltpu.make_async_copy(vw, gvd.at[sp, 1], lsem.at[4]),
        pltpu.make_async_copy(dwt, gvd.at[sp, 2], lsem.at[5]),
        pltpu.make_async_copy(og, ogs, lsem.at[6]),
        pltpu.make_async_copy(wout, wof.at[0], lsem.at[7]),
        pltpu.make_async_copy(res, stream, lsem.at[8]),
    ]
    for load in loads:
        load.start()

    barrier = pltpu.get_barrier_semaphore()
    peers = [partner, nxt, prv]
    for d in (1, 2, 3):
        peers += [dev_x(d), dev_y(d), dev_z(d)]
    for peer in peers:
        pl.semaphore_signal(barrier, inc=1, device_id=peer, device_id_type=MESH)

    pending = []

    def start(copy):
        copy.start()
        pending.append(copy)

    halo = [
        remote(xv.at[pl.ds(ROWS - 16, 16)], xs.at[pl.ds(0, 16)], hsend.at[0], hrecv.at[0], nxt),
        remote(wrt.at[:, pl.ds(ROWS - 128, 128)], bct.at[pl.ds(0, 64), pl.ds(0, 128)], hsend.at[1], hrecv.at[1], nxt),
        remote(rdt.at[:, pl.ds(ROWS - 128, 128)], bct.at[pl.ds(64, 64), pl.ds(0, 128)], hsend.at[2], hrecv.at[2], nxt),
    ]

    @pl.when(sp == 0)
    def _():
        xs[pl.ds(0, 16), :] = jnp.zeros((16, INNER), BF16)
        bct[:, pl.ds(0, 128)] = jnp.zeros((128, 128), BF16)
        fin[pl.ds(0, 16), :] = jnp.zeros((16, WIDTH), BF16)

    def piece(r):
        return remote(
            wout.at[sp, :, pl.ds(0, PLANE)],
            wof.at[r, sp, :, pl.ds(0, PLANE)],
            xsend.at[r - 1],
            xrecv.at[r - 1],
            dev_x(-r),
        )

    def full(batch, k):
        if batch == 0:
            return wof.at[pl.ds(1, 3), k, :, pl.ds(0, PLANE)]
        if batch == 1:
            return gvd.at[k, pl.ds(0, 2)]
        return gvd.at[k, 2]

    def half(batch, k, side):
        if batch == 0:
            return wof.at[pl.ds(1, 3), k, :, pl.ds(PLANE // 2 * side, PLANE // 2)]
        if batch == 1:
            return gvd.at[k, side]
        return gvd.at[k, 2, pl.ds(32 * side, 32)]

    right = pl.ds(PLANE, WIDTH - PLANE)

    def slab(r, core):
        return wof.at[r, pl.ds(pl.multiple_of(16 * core, 16), 16), :, right]

    def slab_half(r, core, side):
        return wof.at[r, pl.ds(pl.multiple_of(16 * core + 8 * side, 8), 8), :, right]

    own_slab = wout.at[pl.ds(pl.multiple_of(16 * c, 16), 16), :, right]
    w_right = remote(own_slab, slab(3, c), vsend.at[0], vrecv.at[0], dev_x(1))
    w_left = remote(own_slab, slab(1, c), vsend.at[1], vrecv.at[1], dev_x(-1))
    w_fright = remote(slab_half(3, c, 0), slab_half(2, c, 0), vsend.at[2], vrecv.at[2], dev_x(1))
    w_fleft = remote(slab_half(1, c, 1), slab_half(2, c, 1), vsend.at[3], vrecv.at[3], dev_x(-1))

    def slab_partner(r):
        return remote(slab(r, c), slab(r, c), vsend.at[3 + r], vrecv.at[3 + r], partner)

    def slab_events():
        w_right.wait_recv()
        start(w_fright)
        start(slab_partner(3))
        w_left.wait_recv()
        start(w_fleft)
        start(slab_partner(1))

    def slab_last():
        w_fright.wait_recv()
        w_fleft.wait_recv()
        start(slab_partner(2))

    def slab_from_partner():
        for r in (1, 2, 3):
            remote(
                slab(r, 1 - c), slab(r, 1 - c), vsend.at[3 + r], vrecv.at[3 + r], partner
            ).wait_recv()

    def send(batch, ref, sem, dev):
        start(remote(ref, ref, wsend.at[batch, sem], wrecv.at[batch, sem], dev))

    def arrive(batch, ref, sem):
        remote(ref, ref, wsend.at[batch, sem], wrecv.at[batch, sem], partner).wait_recv()

    def to_partner(batch, k):
        ref = full(batch, k)
        start(remote(ref, ref, wsend.at[batch, 20 + k // 2], wrecv.at[batch, 20 + k // 2], partner))

    order = (0, -1, 1, 2)

    def first_sends(batch):
        k = item(0, 0)
        send(batch, full(batch, k), 1, dev1(-1))
        send(batch, full(batch, k), 0, dev1(1))

    def second_copies(batch, j):
        ref = full(batch, item(order[j], 0))
        copies = [
            remote(ref, ref, wsend.at[batch, 5 + 4 * j], wrecv.at[batch, 5 + 4 * j], dev2(-1)),
            remote(ref, ref, wsend.at[batch, 4 + 4 * j], wrecv.at[batch, 4 + 4 * j], dev2(1)),
        ]
        pending.extend(copies)
        return copies

    def second_sends(batch, j):
        for copy in second_copies(batch, j):
            copy.start()
        to_partner(batch, item(order[j], 0))

    def first_copies(batch):
        k = item(-1, 0)
        k2 = item(1, 0)
        ref, ref2 = half(batch, k, 0), half(batch, k2, 1)
        copies = [
            remote(ref, ref, wsend.at[batch, 2], wrecv.at[batch, 2], dev1(1)),
            remote(ref2, ref2, wsend.at[batch, 3], wrecv.at[batch, 3], dev1(-1)),
        ]
        pending.extend(copies)
        return copies

    def first_forward(batch, copies):
        arrive(batch, full(batch, item(-1, 0)), 0)
        copies[0].start()
        arrive(batch, full(batch, item(1, 0)), 1)
        copies[1].start()

    def third_event(batch):
        k = item(2, 0)
        arrive(batch, half(batch, k, 0), 2)
        arrive(batch, half(batch, k, 1), 3)
        second_sends(batch, 3)

    def second_events(batch, j):
        base = 4 + 4 * j
        k = item(order[j], -1)
        arrive(batch, full(batch, k), base)
        send(batch, half(batch, k, 0), base + 2, dev2(1))
        to_partner(batch, k)
        k = item(order[j], 1)
        arrive(batch, full(batch, k), base + 1)
        send(batch, half(batch, k, 1), base + 3, dev2(-1))
        to_partner(batch, k)

    def last_events(batch, j):
        base = 4 + 4 * j
        k = item(order[j], 2)
        arrive(batch, half(batch, k, 0), base + 2)
        arrive(batch, half(batch, k, 1), base + 3)
        to_partner(batch, k)

    def from_partner(batch):
        for i in range(16):
            arrive(batch, full(batch, 2 * i + 1 - c), 20 + i)

    head = lax.broadcasted_iota(jnp.int32, (HEADS, 1), 0)
    bias_c = jnp.zeros((HEADS, 1), F32)
    rate_c = jnp.zeros((HEADS, 1), F32)
    for h in range(HEADS):
        bias_c = jnp.where(head == h, bias[h], bias_c)
        rate_c = jnp.where(head == h, hlog[h], rate_c)
    rate_c = jnp.exp(rate_c)
    v = sct[...] + bias_c
    step = jnp.maximum(v, 0.0) + jnp.log1p(jnp.exp(-jnp.abs(v)))
    logd = -step * rate_c + ext[...]
    row_i = lax.broadcasted_iota(jnp.int32, (BLOCK, BLOCK), 0)
    col_i = lax.broadcasted_iota(jnp.int32, (BLOCK, BLOCK), 1)
    upper = (row_i <= col_i).astype(F32)
    for b in range(BLOCKS):
        st_s[b] = step[:, b * BLOCK : (b + 1) * BLOCK]
        cum_s[b] = jnp.dot(
            logd[:, b * BLOCK : (b + 1) * BLOCK], upper, preferred_element_type=F32, precision=HI
        )

    def expand(value):
        parts = []
        for _ in range(3):
            part = value.astype(BF16).astype(F32)
            parts.append(part)
            value = value - part
        columns = jnp.concatenate(parts, axis=0).T.astype(BF16)
        spread = (
            lax.broadcasted_iota(jnp.int32, (3 * HEADS, INNER), 1) // 64
            == lax.broadcasted_iota(jnp.int32, (3 * HEADS, INNER), 0) % HEADS
        )
        return dot(columns, jnp.where(spread, 1.0, 0.0).astype(BF16))

    loads[0].wait()
    loads[1].wait()
    loads[2].wait()
    vt = vtap[...].astype(F32)
    bt = jnp.concatenate([wtap[...].astype(F32).T, rtap[...].astype(F32).T], axis=0)

    def local(b, _):
        r0 = pl.multiple_of(b * BLOCK, BLOCK)
        vals = xs[pl.ds(r0, BLOCK + 16), :].astype(F32)
        conv = vt[3:4] * vals
        for j in range(3):
            conv = conv + vt[j : j + 1] * pltpu.roll(vals, 3 - j, 0)
        xc = silu(conv[16:]).astype(BF16).astype(F32)
        lanes = bct[:, pl.ds(r0, 2 * BLOCK)].astype(F32)
        conv2 = bt[:, 3:4] * lanes
        for j in range(3):
            conv2 = conv2 + bt[:, j : j + 1] * pltpu.roll(lanes, 3 - j, 1)
        bc = silu(conv2[:, BLOCK:])
        wt = bc[:64].astype(BF16)
        rd = bc[64:].T.astype(BF16)
        bt_s[b] = wt
        c_s[b] = rd
        cumx = expand(cum_s[b])
        stepx = expand(st_s[b])
        last = cumx[BLOCK - 1 : BLOCK]
        scaled = (xc * stepx).astype(BF16)
        sc_s[pl.ds(r0, BLOCK), :] = scaled
        tailed = (scaled.astype(F32) * jnp.exp(last - cumx)).astype(BF16)
        ecx_s[pl.ds(r0, BLOCK), :] = jnp.exp(cumx)
        fresh = dot(wt, tailed)
        lb_s[b] = fresh
        pre_s[b] = last
        return 0

    def inner(b, _):
        r0 = pl.multiple_of(b * BLOCK, BLOCK)
        s = dot(c_s[b], bt_s[b])
        cum = cum_s[b]
        cumt = cum.T
        causal = (
            lax.broadcasted_iota(jnp.int32, (BLOCK, BLOCK), 0)
            >= lax.broadcasted_iota(jnp.int32, (BLOCK, BLOCK), 1)
        )
        low = lax.broadcasted_iota(jnp.int32, (BLOCK, BLOCK), 1) < 64
        for p in range(HEADS // 2):
            rhs = sc_s[pl.ds(r0, BLOCK), pl.ds(p * 128, 128)]
            parts = []
            for h in (2 * p, 2 * p + 1):
                spread = jnp.where(causal, cumt[:, h : h + 1] - cum[h : h + 1, :], -jnp.inf)
                parts.append(dot((s * jnp.exp(spread)).astype(BF16), rhs))
            ins_s[pl.ds(r0, BLOCK), pl.ds(p * 128, 128)] = jnp.where(low, parts[0], parts[1])
        return 0

    def put(ref, decay, state):
        ref[pl.ds(0, 64), :] = state.astype(BF16)
        d = jnp.broadcast_to(decay, (16, decay.shape[1]))
        high = d.astype(BF16)
        ref[pl.ds(64, 16), :] = high
        ref[pl.ds(80, 16), :] = (d - high.astype(F32)).astype(BF16)

    def take(ref, cols=slice(None)):
        decay = ref[pl.ds(64, 16), cols].astype(F32) + ref[pl.ds(80, 16), cols].astype(F32)
        return decay[0:1], ref[pl.ds(0, 64), cols].astype(F32)

    def wait_pieces():
        for r in (1, 2, 3):
            piece(r).wait_recv()

    lax.fori_loop(1, 3, local, 0)
    pl.semaphore_wait(barrier, len(peers))

    @pl.when(sp < 31)
    def _():
        for h in halo:
            h.start()

    for r in (1, 2, 3):
        start(piece(r))
    start(w_right)
    start(w_left)
    for i in (3, 4, 5):
        loads[i].wait()
    for batch in (1, 2):
        k = item(0, 0)
        send(batch, full(batch, k), 1, dev1(-1))
        send(batch, full(batch, k), 0, dev1(1))
    lax.fori_loop(3, BLOCKS, local, 0)

    @pl.when(sp > 0)
    def _():
        for h in halo:
            h.wait_recv()

    lax.fori_loop(0, 1, local, 0)
    state = jnp.zeros((64, INNER), F32)
    total_log = jnp.zeros((1, INNER), F32)
    for b in range(BLOCKS):
        fresh, last = lb_s[b], pre_s[b]
        lb_s[b] = state
        pre_s[b] = total_log
        state = state * jnp.exp(last) + fresh
        total_log = total_log + last
    stv[...] = state
    plog[...] = total_log
    put(m1, jnp.exp(total_log), state)
    q0 = remote(m1, r1, ssend.at[0], srecv.at[0], partner)
    start(q0)
    lax.fori_loop(0, 3, inner, 0)
    q0.wait_recv()

    mine = pl.ds(pl.multiple_of(c * 256, 256), 256)
    d_own, s_own = jnp.exp(plog[:, mine]), stv[:, mine]
    d_par, s_par = take(r1, mine)
    is_first = c == 0
    chip_s = jnp.where(is_first, s_own * d_par + s_par, s_par * d_own + s_own)
    put(r2.at[y], d_own * d_par, chip_s)
    for d in (1, 2, 3):
        start(remote(r2.at[y], r2.at[y], ssend.at[d], srecv.at[d], dev_y(d)))
    early = second_copies(1, 0)
    forwards = [first_copies(batch) for batch in range(3)]

    @pl.when(c == 0)
    def _():
        for copy in early:
            copy.start()

    wait_pieces()
    first_sends(0)

    @pl.when(c == 1)
    def _():
        first_forward(1, forwards[1])
        first_forward(2, forwards[2])

    lax.fori_loop(3, BLOCKS, inner, 0)
    for d in (1, 2, 3):
        src = (y + 4 - d) % 4
        remote(r2.at[src], r2.at[src], ssend.at[d], srecv.at[d], dev_y(d)).wait_recv()
    row_d, row_s = take(r2.at[0])
    exc_d = jnp.where(y > 0, row_d, 1.0)
    exc_s = jnp.where(y > 0, row_s, 0.0)
    for i in (1, 2, 3):
        di, si = take(r2.at[i])
        row_s = row_s * di + si
        row_d = row_d * di
        exc_s = jnp.where(y > i, exc_s * di + si, exc_s)
        exc_d = jnp.where(y > i, exc_d * di, exc_d)
    put(r3.at[z], row_d, row_s)
    exc[0] = exc_s
    exc[1] = jnp.broadcast_to(exc_d, (64, 256))
    for d in (1, 2, 3):
        start(remote(r3.at[z], r3.at[z], ssend.at[3 + d], srecv.at[3 + d], dev_z(d)))

    @pl.when(c == 1)
    def _():
        for copy in early:
            copy.start()

    @pl.when(c == 0)
    def _():
        first_forward(1, forwards[1])
        first_forward(2, forwards[2])

    first_forward(0, forwards[0])
    for d in (1, 2, 3):
        src = (z + 4 - d) % 4
        remote(r3.at[src], r3.at[src], ssend.at[3 + d], srecv.at[3 + d], dev_z(d)).wait_recv()
    acc = jnp.zeros((64, 256), F32)
    for i in (0, 1, 2):
        di, si = take(r3.at[i])
        acc = jnp.where(z > i, acc * di + si, acc)
    inc[c] = acc * exc[1] + exc[0]
    q1 = remote(inc.at[c], inc.at[c], ssend.at[7], srecv.at[7], partner)
    start(q1)
    slab_events()
    for j in (0, 1, 2):
        second_sends(0, j)
    remote(inc.at[1 - c], inc.at[1 - c], ssend.at[7], srecv.at[7], partner).wait_recv()
    d_par, s_par = take(r1)
    arrived = jnp.concatenate([inc[0], inc[1]], axis=1)
    stv[...] = jnp.where(is_first, arrived, arrived * d_par + s_par)

    loads[6].wait()
    gain = ggain[...]

    def block_of(i):
        return (i + 4) % 6

    def rows_of(i):
        return pl.multiple_of(block_of(i) * BLOCK, BLOCK)

    def ng_full(r, i):
        return ng.at[r, pl.ds(rows_of(i), BLOCK)]

    def ng_half(r, i, side):
        return ng.at[r, pl.ds(pl.multiple_of(rows_of(i) + 64 * side, 64), 64)]

    def ag_right(i):
        return remote(ng_full(0, i), ng_full(3, i), asend.at[0, i], arecv.at[0, i], dev_x(1))

    def ag_left(i):
        return remote(ng_full(0, i), ng_full(1, i), asend.at[1, i], arecv.at[1, i], dev_x(-1))

    def ag_forward_right(i):
        return remote(ng_half(3, i, 0), ng_half(2, i, 0), asend.at[2, i], arecv.at[2, i], dev_x(1))

    def ag_forward_left(i):
        return remote(ng_half(1, i, 1), ng_half(2, i, 1), asend.at[3, i], arecv.at[3, i], dev_x(-1))

    def final(i, _):
        b = block_of(i)
        r0 = rows_of(i)
        state = lb_s[b] + stv[...] * jnp.exp(pre_s[b])
        ent = dot(c_s[b], state.astype(BF16))
        m = ins_s[pl.ds(r0, BLOCK), :] + ecx_s[pl.ds(r0, BLOCK), :] * ent
        g = m * silu(ogs[pl.ds(r0, BLOCK), :].astype(F32))
        scale = lax.rsqrt(jnp.mean(g * g, axis=-1, keepdims=True) + EPS)
        ng[0, pl.ds(r0, BLOCK), :] = (g * scale * gain).astype(BF16)

        @pl.when((i > 0) & (i < 5))
        def _():
            ag_right(i - 1).start()
            ag_left(i - 1).start()

        return 0

    lax.fori_loop(0, BLOCKS, final, 0)
    third_event(0)

    def ag_forward(i):
        ag_right(i).wait_recv()
        ag_forward_right(i).start()
        ag_left(i).wait_recv()
        ag_forward_left(i).start()

    def ag_last(i):
        ag_forward_right(i).wait_recv()
        ag_forward_left(i).wait_recv()

    to_partner(1, item(0, 0))
    second_sends(1, 1)
    ag_forward(0)
    ag_right(4).start()
    ag_left(4).start()
    for j in range(4):
        second_events(0, j)
    second_sends(1, 2)
    third_event(1)
    ag_forward(1)
    ag_right(5).start()
    ag_left(5).start()
    slab_last()
    ag_forward(2)
    for j in range(4):
        last_events(0, j)
    second_events(1, 0)
    second_sends(2, 0)
    second_sends(2, 1)
    ag_forward(3)
    second_events(1, 1)
    second_events(1, 2)
    loads[7].wait()
    loads[8].wait()

    def project(g):
        ag_last(2 * g)
        ag_last(2 * g + 1)
        r0 = ((g + 2) % 3) * 256

        def tile(n, total):
            n0 = pl.multiple_of(n * 512, 512)
            part = dot(ng[0, pl.ds(r0, 256), :], wof[0, :, :, pl.ds(n0, 512)].reshape(INNER, 512))
            for r in (1, 2, 3):
                part = part + dot(
                    ng[r, pl.ds(r0, 256), :], wof[r, :, :, pl.ds(n0, 512)].reshape(INNER, 512)
                )
            s = (stream[pl.ds(r0, 256), pl.ds(n0, 512)].astype(F32) + part).astype(BF16)
            stream[pl.ds(r0, 256), pl.ds(n0, 512)] = s
            sf = s.astype(F32)
            return total + jnp.sum(sf * sf, axis=-1, keepdims=True)

        total = lax.fori_loop(0, 4, tile, jnp.zeros((256, 1), F32), unroll=True)
        scale = lax.rsqrt(total * (1.0 / WIDTH) + EPS)

        def norm(n, _):
            n0 = pl.multiple_of(n * 256, 256)
            sf = stream[pl.ds(r0, 256), pl.ds(n0, 256)].astype(F32)
            fin[pl.ds(16 + r0, 256), pl.ds(n0, 256)] = (
                sf * scale * fgain[:, pl.ds(n0, 256)]
            ).astype(BF16)
            return 0

        lax.fori_loop(0, 8, norm, 0)

    slab_from_partner()
    from_partner(0)
    project(0)
    rim = remote(fin.at[pl.ds(ROWS, 16)], fin.at[pl.ds(0, 16)], hsend.at[3], hrecv.at[3], nxt)

    @pl.when(sp < 31)
    def _():
        rim.start()

    second_events(1, 3)
    second_sends(2, 2)
    third_event(2)
    ag_forward(4)
    ag_forward(5)
    second_events(2, 0)
    project(1)
    last_events(1, 0)
    last_events(1, 1)
    second_events(2, 1)
    project(2)
    last_events(1, 2)
    last_events(1, 3)
    second_events(2, 2)
    second_events(2, 3)

    @pl.when(sp > 0)
    def _():
        rim.wait_recv()

    from_partner(1)

    def gates(segments):
        at = [pl.multiple_of(d * SHARE + 96 * side, 32) for d, side in segments]

        def product(n, slot):
            n0 = pl.multiple_of(n * 128, 128)
            w = jnp.concatenate(
                [
                    gvd[:, 0, :, pl.ds(n0, 128)].reshape(WIDTH, 128),
                    gvd[:, 1, :, pl.ds(n0, 128)].reshape(WIDTH, 128),
                ],
                axis=1,
            )
            both = jnp.concatenate([fin[pl.ds(f0, 112), :] for f0 in at], axis=0)
            rows[slot] = dot(both, w).astype(BF16)

        def gate(n, slot):
            n0 = pl.multiple_of(n * 128, 128)
            u = rows[slot].astype(F32)
            taps = jnp.concatenate(
                [gtap[:, pl.ds(n0, 128)].astype(F32), vtap2[:, pl.ds(n0, 128)].astype(F32)], axis=1
            )
            conv = taps[2:3] * u
            for j in range(2):
                conv = conv + taps[j : j + 1] * pltpu.roll(u, 2 - j, 0)
            conv = jnp.concatenate([conv[16:112], conv[128:]], axis=0)
            hid[:, pl.ds(n0, 128)] = (silu(conv[:, :128]) * conv[:, 128:]).astype(BF16)

        def tile(i, _):
            gate(2 * i, 0)
            gate(2 * i + 1, 1)
            product(2 * i + 2, 0)
            product(2 * i + 3, 1)
            return 0

        product(0, 0)
        product(1, 1)
        lax.fori_loop(0, 4, tile, 0)
        gate(8, 0)
        gate(9, 1)
        product(10, 0)
        gate(10, 0)

    def downs(first, end, store):
        def down(n, _):
            n0 = pl.multiple_of(n * 512, 512)
            w = gvd[pl.ds(n * 8, 8), 2].reshape(512, HIDDEN)
            store(
                n0,
                lax.dot_general(hid[...], w, (((1,), (1,)), ((), ())), preferred_element_type=F32),
            )
            return 0

        lax.fori_loop(first, end, down, 0, unroll=True)

    def feed(segments, store):
        gates(segments)
        downs(0, 4, store)

    def keep(slot):
        def store(n0, value):
            sbuf[slot, :, pl.ds(n0, 512)] = value.astype(BF16)

        return store

    def add(slot, r0, ref):
        def body(n, _):
            n0 = pl.multiple_of(n * 256, 256)
            sbuf[slot, pl.ds(r0, 96), pl.ds(n0, 256)] = (
                sbuf[slot, pl.ds(r0, 96), pl.ds(n0, 256)].astype(F32) + ref[:, pl.ds(n0, 256)].astype(F32)
            ).astype(BF16)
            return 0

        lax.fori_loop(0, 8, body, 0)

    def top(ref):
        return ref.at[pl.ds(0, 96)]

    def bottom(ref):
        return ref.at[pl.ds(96, 96)]

    gates([((x + 2) % 4, 0), ((x + 2) % 4, 1)])
    for j in range(4):
        last_events(2, j)
    from_partner(2)
    firsts = []
    for i in (0, 1):
        cols = pl.ds(1024 * i, 1024)
        downs(2 * i, 2 * i + 2, keep(0))
        qa = remote(
            sbuf.at[0, pl.ds(0, 96), cols], ra.at[:, cols], qsend.at[2 * i], qrecv.at[2 * i], dev_x(1)
        )
        qb = remote(
            sbuf.at[0, pl.ds(96, 96), cols], rb.at[:, cols], qsend.at[2 * i + 1], qrecv.at[2 * i + 1], dev_x(-1)
        )
        start(qa)
        start(qb)
        firsts.append((qa, qb))
    feed([((x + 1) % 4, 1), ((x + 3) % 4, 0)], keep(1))
    q2 = remote(top(sbuf.at[1]), bottom(rl), qsend.at[4], qrecv.at[4], dev_x(1))
    q4 = remote(bottom(sbuf.at[1]), top(rr), qsend.at[5], qrecv.at[5], dev_x(-1))
    start(q2)
    start(q4)
    feed([((x + 1) % 4, 0), ((x + 3) % 4, 1)], keep(2))
    for qa, _ in firsts:
        qa.wait_recv()
    add(2, 0, ra)
    q3 = remote(top(sbuf.at[2]), top(rl), qsend.at[6], qrecv.at[6], dev_x(1))
    start(q3)
    for _, qb in firsts:
        qb.wait_recv()
    add(2, 96, rb)
    q5 = remote(bottom(sbuf.at[2]), bottom(rr), qsend.at[7], qrecv.at[7], dev_x(-1))
    start(q5)

    def hold(n0, value):
        own[:, pl.ds(n0, 512)] = value

    feed([(x, 0), (x, 1)], hold)
    x0 = pl.multiple_of(x * SHARE, 64)
    q2.wait_recv()
    q3.wait_recv()
    q4.wait_recv()
    q5.wait_recv()

    def finish(n, _):
        n0 = pl.multiple_of(n * 256, 256)
        cols = pl.ds(n0, 256)
        out[:, cols] = (
            stream[pl.ds(x0, SHARE), cols].astype(F32)
            + own[:, cols]
            + rl[:, cols].astype(F32)
            + rr[:, cols].astype(F32)
        ).astype(BF16)
        return 0

    lax.fori_loop(0, 8, finish, 0)

    for copy in pending:
        copy.wait_send()
    for i in range(BLOCKS):
        ag_right(i).wait_send()
        ag_left(i).wait_send()
        ag_forward_right(i).wait_send()
        ag_forward_left(i).wait_send()

    @pl.when(sp < 31)
    def _():
        for h in halo:
            h.wait_send()
        rim.wait_send()


def on_device(
    mixer_value_projection,
    write_vectors_projected,
    read_vectors_projected,
    output_gate_projected,
    step_size_scores,
    position_decay_extra,
    step_size_bias,
    head_decay_logarithm,
    value_filter_taps,
    write_filter_taps,
    read_filter_taps,
    gated_group_norm_gain,
    mixer_output_weight,
    residual,
    feedforward_norm_gain,
    feedforward_gate_weight,
    feedforward_value_weight,
    gate_filter_taps,
    single_value_filter_taps,
    feedforward_down_weight,
):
    args = (
        mixer_value_projection,
        write_vectors_projected.T,
        read_vectors_projected.T,
        output_gate_projected,
        step_size_scores.T,
        position_decay_extra.T,
        step_size_bias,
        head_decay_logarithm,
        value_filter_taps,
        write_filter_taps,
        read_filter_taps,
        gated_group_norm_gain.reshape(1, INNER),
        mixer_output_weight.reshape(32, 16, WIDTH),
        residual,
        feedforward_norm_gain.reshape(1, WIDTH),
        feedforward_gate_weight,
        feedforward_value_weight,
        gate_filter_taps,
        single_value_filter_taps,
        feedforward_down_weight.T,
    )
    hbm = pl.BlockSpec(memory_space=pl.ANY)
    vmem = pl.BlockSpec(memory_space=pltpu.VMEM)
    smem = pl.BlockSpec(memory_space=pltpu.SMEM)
    specs = [hbm, hbm, hbm, hbm, vmem, vmem, smem, smem, vmem, vmem, vmem, vmem, hbm, hbm, vmem, hbm, hbm, vmem, vmem, hbm]
    dma = pltpu.SemaphoreType.DMA
    scratch = [
        pltpu.VMEM((16 + ROWS, INNER), BF16),
        pltpu.VMEM((128, 128 + ROWS), BF16),
        pltpu.VMEM((ROWS, INNER), BF16),
        pltpu.VMEM((BLOCKS, HEADS, BLOCK), F32),
        pltpu.VMEM((BLOCKS, HEADS, BLOCK), F32),
        pltpu.VMEM((BLOCKS, 64, BLOCK), BF16),
        pltpu.VMEM((BLOCKS, BLOCK, 64), BF16),
        pltpu.VMEM((ROWS, INNER), BF16),
        pltpu.VMEM((ROWS, INNER), F32),
        pltpu.VMEM((ROWS, INNER), F32),
        pltpu.VMEM((BLOCKS, 64, INNER), F32),
        pltpu.VMEM((BLOCKS, 1, INNER), F32),
        pltpu.VMEM((64, INNER), F32),
        pltpu.VMEM((1, INNER), F32),
        pltpu.VMEM((96, INNER), BF16),
        pltpu.VMEM((96, INNER), BF16),
        pltpu.VMEM((4, 96, 256), BF16),
        pltpu.VMEM((4, 96, 256), BF16),
        pltpu.VMEM((2, 64, 256), F32),
        pltpu.VMEM((2, 64, 256), F32),
        pltpu.VMEM((4, ROWS, INNER), BF16),
        pltpu.VMEM((ROWS, WIDTH), BF16),
        pltpu.VMEM((16 + ROWS, WIDTH), BF16),
        pltpu.VMEM((4, 32, 16, WIDTH), BF16),
        pltpu.VMEM((32, 3, 64, HIDDEN), BF16),
        pltpu.VMEM((2, SHARE + 32, 256), BF16),
        pltpu.VMEM((SHARE, HIDDEN), BF16),
        pltpu.VMEM((3, SHARE, WIDTH), BF16),
        pltpu.VMEM((96, WIDTH), BF16),
        pltpu.VMEM((96, WIDTH), BF16),
        pltpu.VMEM((SHARE, WIDTH), BF16),
        pltpu.VMEM((SHARE, WIDTH), BF16),
        pltpu.VMEM((SHARE, WIDTH), F32),
        dma((9,)),
        dma((7,)),
        dma((7,)),
        dma((4,)),
        dma((4,)),
        dma((3,)),
        dma((3,)),
        dma((8,)),
        dma((8,)),
        dma((3, 36)),
        dma((3, 36)),
        dma((4, BLOCKS)),
        dma((4, BLOCKS)),
        dma((8,)),
        dma((8,)),
    ]
    return pl.pallas_call(
        kernel,
        out_shape=jax.ShapeDtypeStruct((SHARE, WIDTH), BF16),
        in_specs=specs,
        out_specs=vmem,
        scratch_shapes=scratch,
        compiler_params=pltpu.CompilerParams(
            collective_id=0, has_side_effects=True, vmem_limit_bytes=64 * 1024 * 1024 - 65536
        ),
        name="layer",
    )(*args)


def solution(mesh):
    torus = Mesh(mesh.devices.reshape(4, 4, 2, mesh.shape["tp"]), ("sp_0", "sp_1", "sp_2", "tp"))
    in_specs = (
        P(SP, "tp"),
        P(SP, "tp"),
        P(SP, "tp"),
        P(SP, "tp"),
        P(SP, "tp"),
        P(SP, "tp"),
        P("tp"),
        P("tp"),
        P(None, "tp"),
        P(None, "tp"),
        P(None, "tp"),
        P("tp"),
        P("tp", None),
        P(SP, None),
        P(),
        P(SP, "tp"),
        P(SP, "tp"),
        P(None, "tp"),
        P(None, "tp"),
        P("tp", SP),
    )
    return jax.shard_map(
        on_device, mesh=torus, in_specs=in_specs, out_specs=P(SP_TP, None), check_vma=False
    )
```
